512 devices in a mesh: sp: 64 (over z, y), tp: 8 (over x, core).
Axes of the slice: x: 4, y: 8, z: 8, core: 2. Of those that a mesh axis runs over, the one named last changes fastest.
Arguments:
- tokens: bfloat16 [18432, 4096], P('sp', 'tp'), may hold values from -6 to 6
- doc_ids: int32 [18432], P('sp'), may hold values from 0 to 15, never falling along the last dimension, each value on 1 to 9216 neighbouring positions
- norm_gain: float32 [2, 4096], replicated, may hold values from 0.1 to 1.9
- in_proj: bfloat16 [2, 4096, 4096], P(None, 'sp', 'tp'), may hold values from -0.09375 to 0.09375
- mix_proj: bfloat16 [2, 1024, 4096], P(None, 'sp', 'tp'), may hold values from -0.1875 to 0.1875
- out_scale: float32 [2, 4096], replicated, may hold values from 0.1 to 1.9
Outputs:
- mixed_out: bfloat16 [18432, 4096], P('sp', 'tp')
The draws below stay inside these ranges and needn't reach their ends.
Inputs may be any that keep to these rules, and one draw needn't show every extreme that they name: `doc_ids`: document numbers never fall along the sequence, run from 0 to 15, and each document holds at most 9216 positions.
All inputs are finite; a program needn't handle non-finite values.
Results may differ from the reference program's by a relative error of at most 0.0085.
Values may be sent and summed in bfloat16 or wider, within the bound.
No kernel may reach another device: no remote copies, remote signals or barrier semaphores. Data moves between devices by JAX's collectives and lax.ppermute only.
A program may use at most 128 MiB of HBM per device.

```python
import math
import jax
import jax.numpy as jnp
import numpy as np
from jax import lax

D = 4096
GROUP = 1024
WIN = 16
LAYERS = 2
TOKENS = 18432
DOCS = 16


def block_levels(key, extent, shards, low, largest):
    gain, own = 1.0, jax.random.fold_in(key, 6)
    for dim, shards_of in shards:
        heights = jnp.exp(jax.random.uniform(jax.random.fold_in(own, dim), (shards_of,), jnp.float32, low / len(shards), largest / len(shards)))
        gain = gain * jnp.repeat(heights, extent[dim] // shards_of).reshape([-1 if axis == dim else 1 for axis in range(len(extent))])
    return gain


def length_profile(count, total, most, skew):
    weights = [(1 << 20) // math.isqrt(standing ** skew) + 1 for standing in range(2, count + 1)]
    rest, counts = total - most - (count - 1), [1] * (count - 1)
    while rest > 0:
        free = [i for i in range(count - 1) if counts[i] < most]
        whole, budget = sum([weights[i] for i in free]), rest
        for i in free:
            extra = min(most - counts[i], max(1, budget * weights[i] // whole), rest)
            counts[i] = counts[i] + extra
            rest = rest - extra
    return np.array([most] + counts)


def uneven(stream_key, amount, total, most, slope):
    if amount == 2:
        one = jax.random.randint(stream_key, (), max(1, total - most), min(most, total - 1) + 1)
        return jnp.stack([one, total - one])
    tallies = jnp.asarray(length_profile(amount, total, most, slope), jnp.int32)
    couples = (amount - 1) // 2
    source_of, taker = tallies[1:1 + 2 * couples:2], tallies[2:2 + 2 * couples:2]
    margin = jnp.minimum(source_of - 1, most - taker)
    moved = jax.random.randint(jax.random.fold_in(stream_key, 1), (couples,), 0, 1 << 20) % (margin + 1)
    tallies = tallies.at[1:1 + 2 * couples:2].set(source_of - moved).at[2:2 + 2 * couples:2].set(taker + moved)
    return tallies[jax.random.permutation(jax.random.fold_in(stream_key, 2), amount)]


def scatter_about(rng, dims, spread, limit, shards=(), kind=jnp.bfloat16):
    values = spread * jax.random.normal(rng, dims, jnp.float32)
    if shards:
        values = values * block_levels(rng, dims, shards, -0.22, 0.18)
    return jnp.clip(values, -limit, limit).astype(kind)


def setup_inputs(seed: int = 0) -> dict:
    splits = jax.random.split(jax.random.key(seed), 7)
    tokens = scatter_about(splits[0], (TOKENS, D), 1.0, 6.0, ((0, 64), (1, 8)))
    doc_ids = jnp.searchsorted(jnp.cumsum(uneven(splits[1], DOCS, TOKENS, TOKENS // 2, 1)), jnp.arange(TOKENS), side="right").astype(jnp.int32)
    norm_gain = jnp.clip(1.0 + 0.18 * jax.random.normal(splits[2], (LAYERS, D), jnp.float32), 0.1, 1.9)
    in_proj = scatter_about(splits[3], (LAYERS, D, D), D ** -0.5, 0.09375, ((1, 64), (2, 8)))
    mix_proj = scatter_about(splits[4], (LAYERS, GROUP, D), GROUP ** -0.5, 0.1875, ((1, 64), (2, 8)))
    out_scale = jnp.clip(1.0 + 0.18 * jax.random.normal(splits[5], (LAYERS, D), jnp.float32), 0.1, 1.9)
    return {"tokens": tokens, "doc_ids": doc_ids, "norm_gain": norm_gain, "in_proj": in_proj, "mix_proj": mix_proj, "out_scale": out_scale}


epsilon = 1e-06

def pool_all(proj_f32, doc_ids, windows):
    padded = jnp.concatenate([jnp.zeros((WIN - 1, D), jnp.float32), proj_f32], axis=0)
    padded_docs = jnp.concatenate([jnp.full((WIN - 1,), -1, jnp.int32), doc_ids.astype(jnp.int32)], axis=0)
    window_sum = jnp.zeros_like(proj_f32)
    window_count = jnp.zeros_like(proj_f32)
    for offset in range(WIN):
        begin = WIN - 1 - offset
        shifted = padded[begin:begin + TOKENS]
        same_doc = padded_docs[begin:begin + TOKENS] == doc_ids
        taken = same_doc[:, None] & (offset < windows)[None, :]
        window_sum = window_sum + jnp.where(taken, shifted, jnp.float32(0.0))
        window_count = window_count + taken.astype(jnp.float32)
    return (window_sum / window_count - proj_f32).astype(jnp.bfloat16)

def reference(tokens, doc_ids, norm_gain, in_proj, mix_proj, out_scale):
    block_width = D // 8
    channels = jnp.arange(D, dtype=jnp.int32)
    windows = jnp.left_shift(jnp.int32(2), channels // block_width % 4)
    current = tokens
    for depth_idx in range(LAYERS):
        values = current.astype(jnp.float32)
        scaled = values * lax.rsqrt(lax.optimization_barrier(jnp.mean(values * values, axis=-1, keepdims=True)) + epsilon)
        normed = (scaled * norm_gain[depth_idx][None, :]).astype(jnp.bfloat16)
        projected = jnp.dot(normed, in_proj[depth_idx], preferred_element_type=jnp.float32).astype(jnp.bfloat16)
        pooled = pool_all(projected.astype(jnp.float32), doc_ids, windows)
        blocks_out = [None] * 8
        for group_idx in range(4):
            first = group_idx * block_width
            second = (group_idx + 4) * block_width
            inputs = jnp.concatenate([pooled[:, first:first + block_width], pooled[:, second:second + block_width]], axis=1)
            weights = jnp.concatenate([mix_proj[depth_idx][:, first:first + block_width], mix_proj[depth_idx][:, second:second + block_width]], axis=1)
            result = jnp.dot(inputs, weights, preferred_element_type=jnp.float32)
            blocks_out[group_idx] = result[:, :block_width]
            blocks_out[group_idx + 4] = result[:, block_width:]
        grouped = jnp.concatenate(blocks_out, axis=1)
        current = (grouped * out_scale[depth_idx][None, :]).astype(jnp.bfloat16)
    return current
```

```python
import jax
import jax.numpy as jnp
from jax import lax
from jax.experimental import pallas as pl
from jax.experimental.pallas import tpu as pltpu
from jax.sharding import PartitionSpec as P

D = 4096
WIN = 16
BLOCK = 512
SIDE = 8
IN_ROWS = 64
MIX_ROWS = 16
HALF = 256
EPS = 1e-06

VMEM = pltpu.VMEM
ANY = pl.ANY


def flat_perm(fn):
    pairs = []
    for z in range(SIDE):
        for y in range(SIDE):
            to_z, to_y = fn(z, y)
            pairs.append((z * SIDE + y, (to_z % SIDE) * SIDE + to_y % SIDE))
    return pairs


def y_groups():
    return [[z * SIDE + y for y in range(SIDE)] for z in range(SIDE)]


def z_groups():
    return [[z * SIDE + y for z in range(SIDE)] for y in range(SIDE)]


def spread(x, axis, groups, count):
    copies = jnp.broadcast_to(x, (count, *x.shape))
    return lax.all_to_all(copies, axis, split_axis=0, concat_axis=0, tiled=True, axis_index_groups=groups)


def weight_copies(sources, kind, lo, rows, dest, sems):
    if kind == "whole":
        src = sources[0]
        return [pltpu.make_async_copy(src.at[:, :, pl.ds(lo, rows), :], dest, sems.at[0])]
    first, second = sources
    return [
        pltpu.make_async_copy(
            first.at[:, :, pl.ds(lo, rows), :], dest.at[:, :, :, pl.ds(0, HALF)], sems.at[0]
        )
    ] + [
        pltpu.make_async_copy(
            second.at[y, :, pl.ds(lo, rows), :], dest.at[:, y, :, pl.ds(HALF, HALF)], sems.at[1 + y]
        )
        for y in range(SIDE)
    ]


def project_pool(pieces, order, gain, meta, weights, kind):
    n_x = len(pieces)
    n_w = len(weights)
    rows = pieces[0].shape[1]

    def kernel(*refs):
        order_ref = refs[0]
        x_refs = refs[1 : 1 + n_x]
        gain_ref, meta_ref = refs[1 + n_x : 3 + n_x]
        w_refs = refs[3 + n_x : 3 + n_x + n_w]
        out_ref, w_all, acc, scale, sems = refs[3 + n_x + n_w :]
        copies = weight_copies(w_refs, kind, 0, IN_ROWS, w_all, sems)
        for c in copies:
            c.start()
        total = jnp.zeros((rows, BLOCK), jnp.float32)
        for x_ref in x_refs:
            def add_square(i, total, x_ref=x_ref):
                v = x_ref[i].astype(jnp.float32)
                return total + v * v
            total = lax.fori_loop(0, x_ref.shape[0], add_square, total)
        mean = jnp.sum(total, axis=1, keepdims=True) * (1.0 / D)
        scale[...] = jnp.broadcast_to(lax.rsqrt(mean + EPS), (rows, 128))
        acc[...] = jnp.zeros_like(acc)
        for c in copies:
            c.wait()
        at = 0
        for x_ref in x_refs:
            def step(i, carry, x_ref=x_ref, at=at):
                block = order_ref[at + i]
                v = x_ref[i].astype(jnp.float32)
                normed = v * scale[:, 0:1] * gain_ref[pl.ds(block, 1), :]
                w = w_all[block].reshape(BLOCK, BLOCK)
                acc[...] += jnp.dot(normed.astype(jnp.bfloat16), w, preferred_element_type=jnp.float32)
                return carry
            lax.fori_loop(0, x_ref.shape[0], step, 0)
            at += x_ref.shape[0]
        for c in range(BLOCK // 128):
            lanes = pl.ds(c * 128, 128)
            proj = acc[:, lanes].astype(jnp.bfloat16).astype(jnp.float32)
            total = proj
            for j in range(4):
                moved = pltpu.roll(total, 2**j, 0)
                total = total + jnp.where(meta_ref[j] > 0.0, moved, 0.0)
            pooled = total * meta_ref[4] - proj
            out_ref[:, lanes] = pooled[WIN:].astype(jnp.bfloat16)

    n_sems = 1 if kind == "whole" else 1 + SIDE
    return pl.pallas_call(
        kernel,
        out_shape=jax.ShapeDtypeStruct((rows - WIN, BLOCK), jnp.bfloat16),
        in_specs=[pl.BlockSpec(memory_space=pltpu.SMEM)]
        + [pl.BlockSpec(memory_space=VMEM)] * (n_x + 2)
        + [pl.BlockSpec(memory_space=ANY)] * n_w,
        out_specs=pl.BlockSpec(memory_space=VMEM),
        scratch_shapes=[
            VMEM((SIDE, SIDE, IN_ROWS, BLOCK), jnp.bfloat16),
            VMEM((rows, BLOCK), jnp.float32),
            VMEM((rows, 128), jnp.float32),
            pltpu.SemaphoreType.DMA((n_sems,)),
        ],
        compiler_params=pltpu.CompilerParams(vmem_limit_bytes=40 * 1024 * 1024),
        cost_estimate=pl.CostEstimate(
            flops=2 * rows * D * BLOCK, bytes_accessed=7 * 1024 * 1024, transcendentals=0
        ),
        name="project_pool",
    )(order, *pieces, gain, meta, *weights)


def mix(side, own, other, scale_row, weights, kind):
    n_w = len(weights)
    rows = own.shape[0]

    def kernel(*refs):
        side_ref, own_ref, other_ref, scale_ref = refs[:4]
        w_refs = refs[4 : 4 + n_w]
        out_ref, w_all, sems = refs[4 + n_w :]
        copies = weight_copies(w_refs, kind, IN_ROWS, MIX_ROWS, w_all, sems)
        for c in copies:
            c.start()
        for c in copies:
            c.wait()
        mine = side_ref[0] * (SIDE // 2)
        theirs = (1 - side_ref[0]) * (SIDE // 2)
        w_own = w_all[pl.ds(mine, SIDE // 2)].reshape(BLOCK, BLOCK)
        w_other = w_all[pl.ds(theirs, SIDE // 2)].reshape(BLOCK, BLOCK)
        total = jnp.dot(own_ref[...], w_own, preferred_element_type=jnp.float32)
        total = total + jnp.dot(other_ref[...], w_other, preferred_element_type=jnp.float32)
        out_ref[...] = (total * scale_ref[...]).astype(jnp.bfloat16)

    n_sems = 1 if kind == "whole" else 1 + SIDE
    return pl.pallas_call(
        kernel,
        out_shape=jax.ShapeDtypeStruct((rows, BLOCK), jnp.bfloat16),
        in_specs=[pl.BlockSpec(memory_space=pltpu.SMEM)]
        + [pl.BlockSpec(memory_space=VMEM)] * 3
        + [pl.BlockSpec(memory_space=ANY)] * n_w,
        out_specs=pl.BlockSpec(memory_space=VMEM),
        scratch_shapes=[
            VMEM((SIDE, SIDE, MIX_ROWS, BLOCK), jnp.bfloat16),
            pltpu.SemaphoreType.DMA((n_sems,)),
        ],
        compiler_params=pltpu.CompilerParams(vmem_limit_bytes=24 * 1024 * 1024),
        cost_estimate=pl.CostEstimate(
            flops=4 * rows * BLOCK * BLOCK, bytes_accessed=2 * 1024 * 1024, transcendentals=0
        ),
        name="mix",
    )(side, own, other, scale_row, *weights)


def tp_perm(fn):
    return [(t, fn(t) % 8) for t in range(8)]


def shards(tokens, doc_ids, norm_gain, in_proj, mix_proj, out_scale):
    rows = tokens.shape[0]
    tp = lax.axis_index("tp")
    sp = lax.axis_index("sp")
    first = sp == 0
    per_layer = jnp.concatenate([in_proj, mix_proj], axis=1)

    w1 = lax.all_gather(per_layer[1], "sp", axis=0, tiled=True)
    w1 = w1.reshape(SIDE, SIDE, IN_ROWS + MIX_ROWS, BLOCK)

    both = IN_ROWS + MIX_ROWS
    left = spread(per_layer[0, :, :HALF], "sp", y_groups(), SIDE)
    right = spread(per_layer[0, :, HALF:], "sp", z_groups(), SIDE)
    left = spread(left.reshape(SIDE * both, HALF), "sp", z_groups(), SIDE)
    right = spread(right.reshape(SIDE * both, HALF), "sp", y_groups(), SIDE)
    left = left.reshape(SIDE, SIDE, both, HALF)
    right = right.reshape(SIDE, SIDE, both, HALF)

    halo = 2 * WIN
    flags = (doc_ids + 1).astype(jnp.bfloat16)
    flag_row = jnp.pad(flags[rows - halo :], (0, BLOCK - halo)).reshape(1, BLOCK)
    tail = jnp.concatenate([tokens[rows - halo :], jnp.pad(flag_row, ((0, 15), (0, 0)))], axis=0)
    route = [(i, i + 1) for i in range(SIDE * SIDE - 1)]
    tail = lax.ppermute(tail, "sp", route)
    ext_tokens = jnp.concatenate([tail[:halo], tokens], axis=0)
    ext_docs = jnp.concatenate([tail[halo, :halo], flags], axis=0).astype(jnp.float32)

    window = jnp.left_shift(jnp.int32(2), tp % 4)
    masks, run = [], jnp.ones_like(ext_docs)
    for offset in range(1, WIN):
        same = jnp.pad(ext_docs[:-offset], (offset, 0)) == ext_docs
        same = same & (offset < window)
        run = run + same.astype(jnp.float32)
        if offset in (1, 2, 4, 8):
            masks.append(same.astype(jnp.float32))
    meta = jnp.stack(masks + [1.0 / run], axis=0)
    meta = jnp.broadcast_to(meta[:, :, None], (5, rows + halo, 128))

    side = (tp // 4).reshape(1).astype(jnp.int32)
    gain = norm_gain.reshape(2, 8, BLOCK)
    scale = lax.dynamic_slice(out_scale, (0, tp * BLOCK), (2, BLOCK))
    partner = tp_perm(lambda t: t ^ 4)

    gathered = spread(ext_tokens, "tp", None, 8)
    pooled = project_pool(
        [gathered], jnp.arange(8, dtype=jnp.int32), gain[0], meta, [left, right], "halves"
    )
    other = lax.ppermute(pooled, "tp", partner)
    current = mix(side, pooled, other, scale[0:1], [left, right], "halves")

    arrived = [current] + [lax.ppermute(current, "tp", tp_perm(lambda t, k=k: t - 2 * k)) for k in (1, 2, 3)]
    mine = jnp.stack(arrived, axis=0)
    theirs = lax.ppermute(mine, "tp", tp_perm(lambda t: t ^ 1))
    hops = (jnp.arange(4, dtype=jnp.int32) + tp // 2) % 4
    order = jnp.concatenate([2 * hops + tp % 2, 2 * hops + 1 - tp % 2])
    pooled = project_pool([mine, theirs], order, gain[1], meta[:, WIN:], [w1], "whole")
    other = lax.ppermute(pooled, "tp", partner)
    return mix(side, pooled, other, scale[1:2], [w1], "whole")


def solution(mesh):
    placed = (P("sp", "tp"), P("sp"), P(), P(None, "sp", "tp"), P(None, "sp", "tp"), P())
    return jax.shard_map(
        shards, mesh=mesh, in_specs=placed, out_specs=P("sp", "tp"), check_vma=False
    )
```

```python
import jax
import jax.numpy as jnp
from jax import lax
from jax.experimental import pallas as pl
from jax.experimental.pallas import tpu as pltpu
from jax.sharding import PartitionSpec as P


D = 4096
WIN = 16
BLOCK = 512
SIDE = 8
IN_ROWS = 64
MIX_ROWS = 16
BOTH = IN_ROWS + MIX_ROWS
EPS = 1e-06

VMEM = pltpu.VMEM


def device(z, y, t):
    return ((z % SIDE) * SIDE + y % SIDE) * 8 + t


EVERY = [(z, y, t) for z in range(SIDE) for y in range(SIDE) for t in range(8)]


def short_groups():
    groups = []
    for t in range(8):
        for a in range(SIDE):
            groups.append([device(b, a, t) if t % 2 else device(a, b, t) for b in range(SIDE)])
    return groups


def long_shift(distance):
    return [
        (device(z, y + distance, t) if t % 2 else device(z + distance, y, t), device(z, y, t))
        for z, y, t in EVERY
    ]


def tp_perm(fn):
    return [(t, fn(t) % 8) for t in range(8)]


def weight_copies(pieces, lo, rows, dest, place, sems):
    if len(pieces) == 1:
        return [pltpu.make_async_copy(pieces[0].at[:, :, pl.ds(lo, rows), :], dest, sems.at[0])]
    return [
        pltpu.make_async_copy(
            piece.at[:, pl.ds(lo, rows), :], dest.at[lax.rem(place + k, SIDE)], sems.at[k]
        )
        for k, piece in enumerate(pieces)
    ]


STRIDE_Z, STRIDE_Y, PLACE, SIDE_OF, WINDOW = 8, 9, 10, 11, 12


def project_pool(pieces, info, gain, docs, weights):
    n_x = len(pieces)
    n_w = len(weights)
    rows = pieces[0].shape[1]

    def kernel(*refs):
        info_ref = refs[0]
        x_refs = refs[1 : 1 + n_x]
        gain_ref, docs_ref = refs[1 + n_x : 3 + n_x]
        w_refs = refs[3 + n_x : 3 + n_x + n_w]
        out_ref, w_all, acc, scale, sems = refs[3 + n_x + n_w :]
        copies = weight_copies(w_refs, 0, IN_ROWS, w_all, info_ref[PLACE], sems)
        for c in copies:
            c.start()
        total = jnp.zeros((rows, BLOCK), jnp.float32)
        for x_ref in x_refs:
            def add_square(i, total, x_ref=x_ref):
                v = x_ref[i].astype(jnp.float32)
                return total + v * v
            total = lax.fori_loop(0, x_ref.shape[0], add_square, total)
        mean = jnp.sum(total, axis=1, keepdims=True) * (1.0 / D)
        scale[...] = jnp.broadcast_to(lax.rsqrt(mean + EPS), (rows, 128))
        acc[...] = jnp.zeros_like(acc)
        for c in copies:
            c.wait()
        flat = w_all.reshape(SIDE * SIDE, IN_ROWS, BLOCK)
        at = 0
        for x_ref in x_refs:
            def step(i, carry, x_ref=x_ref, at=at):
                block = info_ref[at + i]
                v = x_ref[i].astype(jnp.float32)
                normed = v * scale[:, 0:1] * gain_ref[pl.ds(block, 1), :]
                w = jnp.concatenate(
                    [flat[info_ref[STRIDE_Z] * block + info_ref[STRIDE_Y] * y] for y in range(SIDE)],
                    axis=0,
                )
                acc[...] += jnp.dot(normed.astype(jnp.bfloat16), w, preferred_element_type=jnp.float32)
                return carry
            lax.fori_loop(0, x_ref.shape[0], step, 0)
            at += x_ref.shape[0]
        own = docs_ref[...]
        masks, count = [], jnp.ones_like(own)
        for j in range(4):
            taken = (pltpu.roll(own, 2**j, 0) == own) & (2**j < info_ref[WINDOW])
            masks.append(taken)
            count = count + jnp.where(taken, pltpu.roll(count, 2**j, 0), 0.0)
        share = 1.0 / count
        for c in range(BLOCK // 128):
            lanes = pl.ds(c * 128, 128)
            proj = acc[:, lanes].astype(jnp.bfloat16).astype(jnp.float32)
            total = proj
            for j in range(4):
                total = total + jnp.where(masks[j], pltpu.roll(total, 2**j, 0), 0.0)
            pooled = total * share - proj
            out_ref[:, lanes] = pooled[WIN:].astype(jnp.bfloat16)

    return pl.pallas_call(
        kernel,
        out_shape=jax.ShapeDtypeStruct((rows - WIN, BLOCK), jnp.bfloat16),
        in_specs=[pl.BlockSpec(memory_space=pltpu.SMEM)]
        + [pl.BlockSpec(memory_space=VMEM)] * (n_x + 2)
        + [pl.BlockSpec(memory_space=pltpu.HBM)] * n_w,
        out_specs=pl.BlockSpec(memory_space=VMEM),
        scratch_shapes=[
            VMEM((SIDE, SIDE, IN_ROWS, BLOCK), jnp.bfloat16),
            VMEM((rows, BLOCK), jnp.float32),
            VMEM((rows, 128), jnp.float32),
            pltpu.SemaphoreType.DMA((n_w,)),
        ],
        compiler_params=pltpu.CompilerParams(vmem_limit_bytes=40 * 1024 * 1024),
        cost_estimate=pl.CostEstimate(
            flops=2 * rows * D * BLOCK, bytes_accessed=7 * 1024 * 1024, transcendentals=0
        ),
        name="project_pool",
    )(info, *pieces, gain, docs, *weights)


def mix(own, other, info, scale_row, weights):
    n_w = len(weights)
    rows = own.shape[0]

    def kernel(*refs):
        info_ref, own_ref, other_ref, scale_ref = refs[:4]
        w_refs = refs[4 : 4 + n_w]
        out_ref, w_all, sems = refs[4 + n_w :]
        copies = weight_copies(w_refs, IN_ROWS, MIX_ROWS, w_all, info_ref[PLACE], sems)
        for c in copies:
            c.start()
        for c in copies:
            c.wait()
        flat = w_all.reshape(SIDE * SIDE, MIX_ROWS, BLOCK)

        def half(side):
            return jnp.concatenate(
                [
                    flat[info_ref[STRIDE_Z] * (4 * side + z) + info_ref[STRIDE_Y] * y]
                    for z in range(SIDE // 2)
                    for y in range(SIDE)
                ],
                axis=0,
            )

        side = info_ref[SIDE_OF]
        total = jnp.dot(own_ref[...], half(side), preferred_element_type=jnp.float32)
        total = total + jnp.dot(other_ref[...], half(1 - side), preferred_element_type=jnp.float32)
        out_ref[...] = (total * scale_ref[...]).astype(jnp.bfloat16)

    return pl.pallas_call(
        kernel,
        out_shape=jax.ShapeDtypeStruct((rows, BLOCK), jnp.bfloat16),
        in_specs=[pl.BlockSpec(memory_space=pltpu.SMEM)]
        + [pl.BlockSpec(memory_space=VMEM)] * 3
        + [pl.BlockSpec(memory_space=pltpu.HBM)] * n_w,
        out_specs=pl.BlockSpec(memory_space=VMEM),
        scratch_shapes=[
            VMEM((SIDE, SIDE, MIX_ROWS, BLOCK), jnp.bfloat16),
            pltpu.SemaphoreType.DMA((n_w,)),
        ],
        compiler_params=pltpu.CompilerParams(vmem_limit_bytes=24 * 1024 * 1024),
        cost_estimate=pl.CostEstimate(
            flops=4 * rows * BLOCK * BLOCK, bytes_accessed=2 * 1024 * 1024, transcendentals=0
        ),
        name="mix",
    )(info, own, other, scale_row, *weights)


def all_channels(x):
    arrived = [x] + [lax.ppermute(x, "tp", tp_perm(lambda t, k=k: t - 2 * k)) for k in (1, 2, 3)]
    mine = jnp.stack(arrived, axis=0)
    theirs = lax.ppermute(mine, "tp", tp_perm(lambda t: t ^ 1))
    return [mine, theirs]


def shards(tokens, doc_ids, norm_gain, in_proj, mix_proj, out_scale):
    rows = tokens.shape[0]
    tp = lax.axis_index("tp")
    sp = lax.axis_index("sp")
    chip, core = tp // 2, tp % 2
    both_axes = ("sp", "tp")

    w1 = jnp.concatenate([in_proj[1], mix_proj[1]], axis=0)
    w1 = lax.all_gather(w1, "sp", axis=0, tiled=True)
    w1 = w1.reshape(SIDE, SIDE, BOTH, BLOCK)

    w0 = jnp.concatenate([in_proj[0], mix_proj[0]], axis=0)
    w0 = lax.ppermute(w0, "tp", tp_perm(lambda t: 2 * (t % 4) + t // 4))
    w0 = jnp.broadcast_to(w0, (SIDE, BOTH, BLOCK))
    w0 = lax.all_to_all(
        w0, both_axes, split_axis=0, concat_axis=0, tiled=True, axis_index_groups=short_groups()
    )
    up, down = [w0], [w0]
    for step in range(3):
        up.append(lax.ppermute(up[-1], both_axes, long_shift(1)))
        down.append(lax.ppermute(down[-1], both_axes, long_shift(-1)))
    far = lax.ppermute(up[3], both_axes, long_shift(1))
    w0 = up + [far] + down[3:0:-1]

    halo = 2 * WIN
    flags = (doc_ids + 1).astype(jnp.bfloat16)
    flag_row = jnp.pad(flags[rows - halo :], (0, BLOCK - halo)).reshape(1, BLOCK)
    tail = jnp.concatenate([tokens[rows - halo :], jnp.pad(flag_row, ((0, 15), (0, 0)))], axis=0)
    route = [(i, i + 1) for i in range(SIDE * SIDE - 1)]
    tail = lax.ppermute(tail, "sp", route)
    ext_tokens = jnp.concatenate([tail[:halo], tokens], axis=0)
    docs = jnp.concatenate([tail[halo, :halo], flags], axis=0).astype(jnp.float32)
    docs = jnp.broadcast_to(docs[:, None], (rows + halo, 128))

    gain = norm_gain.reshape(2, 8, BLOCK)
    hops = (jnp.arange(4, dtype=jnp.int32) + chip) % 4
    zero = jnp.int32(0)

    block = chip + 4 * core
    order = jnp.concatenate([2 * hops + core, 2 * hops + 1 - core])
    window = jnp.left_shift(jnp.int32(2), block % 4)
    place = jnp.where(core == 0, sp // SIDE, sp % SIDE)
    layout = [jnp.where(core == 0, 8, 1), jnp.where(core == 0, 1, 8), place, core, window]
    info = jnp.concatenate([order, jnp.stack([v.astype(jnp.int32) for v in layout])])
    scale = lax.dynamic_slice(out_scale[0:1], (0, block * BLOCK), (1, BLOCK))
    pooled = project_pool(all_channels(ext_tokens), info, gain[0], docs, w0)
    other = lax.ppermute(pooled, "tp", tp_perm(lambda t: t ^ 1))
    current = mix(pooled, other, info, scale, w0)

    order = jnp.concatenate([hops + 4 * core, hops + 4 - 4 * core])
    window = jnp.left_shift(jnp.int32(2), tp % 4)
    layout = [zero + 8, zero + 1, zero, tp // 4, window]
    info = jnp.concatenate([order, jnp.stack([v.astype(jnp.int32) for v in layout])])
    scale = lax.dynamic_slice(out_scale[1:2], (0, tp * BLOCK), (1, BLOCK))
    pooled = project_pool(all_channels(current), info, gain[1], docs[WIN:], [w1])
    other = lax.ppermute(pooled, "tp", tp_perm(lambda t: t ^ 4))
    return mix(pooled, other, info, scale, [w1])


def solution(mesh):
    placed = (P("sp", "tp"), P("sp"), P(), P(None, "sp", "tp"), P(None, "sp", "tp"), P())
    return jax.shard_map(
        shards, mesh=mesh, in_specs=placed, out_specs=P("sp", "tp"), check_vma=False
    )
```

```python
import jax
import jax.numpy as jnp
from jax import lax
from jax.experimental import pallas as pl
from jax.experimental.pallas import tpu as pltpu
from jax.sharding import PartitionSpec as P


D = 4096
WIN = 16
BLOCK = 512
SIDE = 8
IN_ROWS = 64
MIX_ROWS = 16
BOTH = IN_ROWS + MIX_ROWS
EPS = 1e-06

VMEM = pltpu.VMEM


def device(z, y, t):
    return ((z % SIDE) * SIDE + y % SIDE) * 8 + t


EVERY = [(z, y, t) for z in range(SIDE) for y in range(SIDE) for t in range(8)]


def short_groups():
    groups = []
    for t in range(8):
        for a in range(SIDE):
            groups.append([device(b, a, t) if t % 2 else device(a, b, t) for b in range(SIDE)])
    return groups


def long_shift(distance):
    return [
        (device(z, y + distance, t) if t % 2 else device(z + distance, y, t), device(z, y, t))
        for z, y, t in EVERY
    ]


def tp_perm(fn):
    return [(t, fn(t) % 8) for t in range(8)]


CORE, PLACE, SIDE_OF, WINDOW = 8, 9, 10, 11


def fetch(info_ref, pieces, lo, rows, dest, sems):
    if len(pieces) == 1:
        copies = [pltpu.make_async_copy(pieces[0].at[:, :, pl.ds(lo, rows), :], dest, sems.at[0])]
        copies[0].start()
        return copies
    along_z, along_y = [], []
    for k, piece in enumerate(pieces):
        src, at = piece.at[:, pl.ds(lo, rows), :], lax.rem(info_ref[PLACE] + k, SIDE)
        along_z.append(pltpu.make_async_copy(src, dest.at[at], sems.at[k]))
        along_y.append(pltpu.make_async_copy(src, dest.at[:, at], sems.at[k]))

    @pl.when(info_ref[CORE] == 0)
    def _():
        for c in along_z:
            c.start()

    @pl.when(info_ref[CORE] == 1)
    def _():
        for c in along_y:
            c.start()

    return along_z


def write_normed(info_ref, x_refs, gain_ref, dest, rows):
    def chunk(r, carry):
        here = pl.ds(pl.multiple_of(r * 16, 16), 16)
        values = [x_ref[i, here, :].astype(jnp.float32) for x_ref in x_refs for i in range(4)]
        total = values[0] * values[0]
        for v in values[1:]:
            total = total + v * v
        mean = jnp.sum(total, axis=1, keepdims=True) * (1.0 / D)
        scale = lax.rsqrt(mean + EPS)
        for i, v in enumerate(values):
            block = info_ref[i]
            normed = (v * scale) * gain_ref[pl.ds(block, 1), :]
            lanes = pl.ds(pl.multiple_of(block * BLOCK, BLOCK), BLOCK)
            dest[here, lanes] = normed.astype(jnp.bfloat16)
        return carry

    lax.fori_loop(0, rows // 16, chunk, 0)


def normalize(pieces, info, gain):
    rows = pieces[0].shape[1]

    def kernel(info_ref, mine_ref, theirs_ref, gain_ref, out_ref):
        write_normed(info_ref, [mine_ref, theirs_ref], gain_ref, out_ref, rows)

    return pl.pallas_call(
        kernel,
        out_shape=jax.ShapeDtypeStruct((rows, D), jnp.bfloat16),
        in_specs=[pl.BlockSpec(memory_space=pltpu.SMEM)] + [pl.BlockSpec(memory_space=VMEM)] * 3,
        out_specs=pl.BlockSpec(memory_space=VMEM),
        compiler_params=pltpu.CompilerParams(vmem_limit_bytes=16 * 1024 * 1024),
        cost_estimate=pl.CostEstimate(
            flops=200 * rows * D, bytes_accessed=4 * rows * D, transcendentals=0
        ),
        name="normalize",
    )(info, *pieces, gain)


def project_pool(xs, info, gain, docs, weights, limit):
    n_x = len(xs)
    n_w = len(weights)
    rows = docs.shape[0]
    scratch = [
        VMEM((SIDE, SIDE, IN_ROWS, BLOCK), jnp.bfloat16),
        VMEM((rows, BLOCK), jnp.float32),
        pltpu.SemaphoreType.DMA((2, n_w)),
    ]
    if n_x > 1:
        scratch.append(VMEM((rows, D), jnp.bfloat16))

    def kernel(*refs):
        info_ref = refs[0]
        x_refs = refs[1 : 1 + n_x]
        gain_ref, docs_ref = refs[1 + n_x : 3 + n_x]
        w_refs = refs[3 + n_x : 3 + n_x + n_w]
        out_ref, m_ref, w_all, acc, sems = refs[3 + n_x + n_w : 8 + n_x + n_w]
        copies = fetch(info_ref, w_refs, 0, IN_ROWS, w_all, sems.at[0])
        m_copies = fetch(info_ref, w_refs, IN_ROWS, MIX_ROWS, m_ref, sems.at[1])
        if n_x > 1:
            normed = refs[-1]
            write_normed(info_ref, x_refs, gain_ref, normed, rows)
        else:
            normed = x_refs[0]
        for c in copies:
            c.wait()
        for n in range(2):
            lanes = pl.ds(n * 256, 256)
            total = None
            for k in range(8):
                part = jnp.dot(
                    normed[:, k * BLOCK : (k + 1) * BLOCK],
                    w_all[k, :, :, lanes].reshape(BLOCK, 256),
                    preferred_element_type=jnp.float32,
                )
                total = part if total is None else total + part
            acc[:, lanes] = total
        own = docs_ref[...]
        masks, count = [], jnp.ones_like(own)
        for j in range(4):
            taken = (pltpu.roll(own, 2**j, 0) == own) & (2**j < info_ref[WINDOW])
            masks.append(taken)
            count = count + jnp.where(taken, pltpu.roll(count, 2**j, 0), 0.0)
        share = 1.0 / count
        for c in range(BLOCK // 128):
            lanes = pl.ds(c * 128, 128)
            proj = acc[:, lanes].astype(jnp.bfloat16).astype(jnp.float32)
            total = proj
            for j in range(4):
                total = total + jnp.where(masks[j], pltpu.roll(total, 2**j, 0), 0.0)
            pooled = total * share - proj
            out_ref[:, lanes] = pooled[WIN:].astype(jnp.bfloat16)
        for c in m_copies:
            c.wait()

    return pl.pallas_call(
        kernel,
        out_shape=[
            jax.ShapeDtypeStruct((rows - WIN, BLOCK), jnp.bfloat16),
            jax.ShapeDtypeStruct((SIDE, SIDE, MIX_ROWS, BLOCK), jnp.bfloat16),
        ],
        in_specs=[pl.BlockSpec(memory_space=pltpu.SMEM)]
        + [pl.BlockSpec(memory_space=VMEM)] * (n_x + 2)
        + [pl.BlockSpec(memory_space=pltpu.HBM)] * n_w,
        out_specs=[pl.BlockSpec(memory_space=VMEM)] * 2,
        scratch_shapes=scratch,
        compiler_params=pltpu.CompilerParams(vmem_limit_bytes=limit * 1024 * 1024),
        cost_estimate=pl.CostEstimate(
            flops=2 * rows * D * BLOCK, bytes_accessed=7 * 1024 * 1024, transcendentals=0
        ),
        name="project_pool",
    )(info, *xs, gain, docs, *weights)


def mix(own, other, info, scale_row, weights):
    rows = own.shape[0]

    def kernel(info_ref, own_ref, other_ref, scale_ref, w_ref, out_ref):
        side = info_ref[SIDE_OF]
        w_own = w_ref[pl.ds(4 * side, 4)].reshape(BLOCK, BLOCK)
        w_other = w_ref[pl.ds(4 * (1 - side), 4)].reshape(BLOCK, BLOCK)
        total = jnp.dot(own_ref[...], w_own, preferred_element_type=jnp.float32)
        total = total + jnp.dot(other_ref[...], w_other, preferred_element_type=jnp.float32)
        out_ref[...] = (total * scale_ref[...]).astype(jnp.bfloat16)

    return pl.pallas_call(
        kernel,
        out_shape=jax.ShapeDtypeStruct((rows, BLOCK), jnp.bfloat16),
        in_specs=[pl.BlockSpec(memory_space=pltpu.SMEM)] + [pl.BlockSpec(memory_space=VMEM)] * 4,
        out_specs=pl.BlockSpec(memory_space=VMEM),
        compiler_params=pltpu.CompilerParams(vmem_limit_bytes=16 * 1024 * 1024),
        cost_estimate=pl.CostEstimate(
            flops=4 * rows * BLOCK * BLOCK, bytes_accessed=2 * 1024 * 1024, transcendentals=0
        ),
        name="mix",
    )(info, own, other, scale_row, weights)


def all_channels(x):
    arrived = [x]
    for k in (1, 2, 3):
        arrived.append(lax.ppermute(x, "tp", tp_perm(lambda t, k=k: t - 2 * k)))
    mine = jnp.stack(arrived, axis=0)
    theirs = lax.ppermute(mine, "tp", tp_perm(lambda t: t ^ 1))
    return [mine, theirs]


def shards(tokens, doc_ids, norm_gain, in_proj, mix_proj, out_scale):
    rows = tokens.shape[0]
    tp = lax.axis_index("tp")
    sp = lax.axis_index("sp")
    chip, core = tp // 2, tp % 2
    both_axes = ("sp", "tp")

    w1 = jnp.concatenate([in_proj[1], mix_proj[1]], axis=0)
    w1 = lax.all_gather(w1, "sp", axis=0, tiled=True)
    w1 = w1.reshape(SIDE, SIDE, BOTH, BLOCK)

    w0 = jnp.concatenate([in_proj[0], mix_proj[0]], axis=0)
    w0 = lax.ppermute(w0, "tp", tp_perm(lambda t: 2 * (t % 4) + t // 4))
    w0 = jnp.broadcast_to(w0, (SIDE, BOTH, BLOCK))
    w0 = lax.all_to_all(
        w0, both_axes, split_axis=0, concat_axis=0, tiled=True, axis_index_groups=short_groups()
    )
    up, down = [w0], [w0]
    for _ in range(3):
        up.append(lax.ppermute(up[-1], both_axes, long_shift(1)))
        down.append(lax.ppermute(down[-1], both_axes, long_shift(-1)))
    far = lax.ppermute(up[3], both_axes, long_shift(1))
    w0 = up + [far] + down[3:0:-1]

    halo = 2 * WIN
    flags = (doc_ids + 1).astype(jnp.bfloat16)
    flag_row = jnp.pad(flags[rows - halo :], (0, BLOCK - halo)).reshape(1, BLOCK)
    tail = jnp.concatenate([tokens[rows - halo :], jnp.pad(flag_row, ((0, 15), (0, 0)))], axis=0)
    route = [(i, i + 1) for i in range(SIDE * SIDE - 1)]
    tail = lax.ppermute(tail, "sp", route)
    ext_tokens = jnp.concatenate([tail[:halo], tokens], axis=0)
    docs = jnp.concatenate([tail[halo, :halo], flags], axis=0).astype(jnp.float32)
    docs = jnp.broadcast_to(docs[:, None], (rows + halo, 128))

    gain = norm_gain.reshape(2, 8, BLOCK)
    hops = (jnp.arange(4, dtype=jnp.int32) + chip) % 4
    zero = jnp.int32(0)

    block = chip + 4 * core
    order = jnp.concatenate([2 * hops + core, 2 * hops + 1 - core])
    window = jnp.left_shift(jnp.int32(2), block % 4)
    place = jnp.where(core == 0, sp // SIDE, sp % SIDE)
    layout = [core, place, core, window]
    info = jnp.concatenate([order, jnp.stack([v.astype(jnp.int32) for v in layout])])
    scale = lax.dynamic_slice(out_scale[0:1], (0, block * BLOCK), (1, BLOCK))
    normed = normalize(all_channels(ext_tokens), info, gain[0])
    pooled, mix_rows = project_pool([normed], info, gain[0], docs, w0, 24)
    other = lax.ppermute(pooled, "tp", tp_perm(lambda t: t ^ 1))
    current = mix(pooled, other, info, scale, mix_rows)

    order = jnp.concatenate([hops + 4 * core, hops + 4 - 4 * core])
    window = jnp.left_shift(jnp.int32(2), tp % 4)
    layout = [zero, zero, tp // 4, window]
    info = jnp.concatenate([order, jnp.stack([v.astype(jnp.int32) for v in layout])])
    scale = lax.dynamic_slice(out_scale[1:2], (0, tp * BLOCK), (1, BLOCK))
    pooled, mix_rows = project_pool(all_channels(current), info, gain[1], docs[WIN:], [w1], 58)
    other = lax.ppermute(pooled, "tp", tp_perm(lambda t: t ^ 4))
    return mix(pooled, other, info, scale, mix_rows)


def solution(mesh):
    placed = (P("sp", "tp"), P("sp"), P(), P(None, "sp", "tp"), P(None, "sp", "tp"), P())
    return jax.shard_map(
        shards, mesh=mesh, in_specs=placed, out_specs=P("sp", "tp"), check_vma=False
    )
```

```python
import jax
import jax.numpy as jnp
from jax import lax
from jax.experimental import pallas as pl
from jax.experimental.pallas import tpu as pltpu
from jax.sharding import PartitionSpec as P


D = 4096
WIN = 16
BLOCK = 512
SIDE = 8
IN_ROWS = 64
MIX_ROWS = 16
BOTH = IN_ROWS + MIX_ROWS
EPS = 1e-06

VMEM = pltpu.VMEM


def device(z, y, t):
    return ((z % SIDE) * SIDE + y % SIDE) * 8 + t


EVERY = [(z, y, t) for z in range(SIDE) for y in range(SIDE) for t in range(8)]


def short_groups():
    groups = []
    for t in range(8):
        for a in range(SIDE):
            groups.append([device(b, a, t) if t % 2 else device(a, b, t) for b in range(SIDE)])
    return groups


def long_shift(distance):
    return [
        (device(z, y + distance, t) if t % 2 else device(z + distance, y, t), device(z, y, t))
        for z, y, t in EVERY
    ]


def tp_perm(fn):
    return [(t, fn(t) % 8) for t in range(8)]


CORE, PLACE, SIDE_OF, WINDOW = 8, 9, 10, 11


def fetch(info_ref, pieces, lo, rows, dest, sems):
    if len(pieces) == 1:
        copies = [pltpu.make_async_copy(pieces[0].at[:, :, pl.ds(lo, rows), :], dest, sems.at[0])]
        copies[0].start()
        return copies
    along_z, along_y = [], []
    for k, piece in enumerate(pieces):
        src, at = piece.at[:, pl.ds(lo, rows), :], lax.rem(info_ref[PLACE] + k, SIDE)
        along_z.append(pltpu.make_async_copy(src, dest.at[at], sems.at[k]))
        along_y.append(pltpu.make_async_copy(src, dest.at[:, at], sems.at[k]))

    @pl.when(info_ref[CORE] == 0)
    def _():
        for c in along_z:
            c.start()

    @pl.when(info_ref[CORE] == 1)
    def _():
        for c in along_y:
            c.start()

    return along_z


def write_normed(info_ref, x_refs, gain_ref, dest, rows):
    def chunk(r, carry):
        here = pl.ds(pl.multiple_of(r * 16, 16), 16)
        values = [x_ref[i, here, :].astype(jnp.float32) for x_ref in x_refs for i in range(4)]
        total = values[0] * values[0]
        for v in values[1:]:
            total = total + v * v
        mean = jnp.sum(total, axis=1, keepdims=True) * (1.0 / D)
        scale = lax.rsqrt(mean + EPS)
        for i, v in enumerate(values):
            block = info_ref[i]
            normed = (v * scale) * gain_ref[pl.ds(block, 1), :]
            lanes = pl.ds(pl.multiple_of(block * BLOCK, BLOCK), BLOCK)
            dest[here, lanes] = normed.astype(jnp.bfloat16)
        return carry

    lax.fori_loop(0, rows // 16, chunk, 0)


def normalize(pieces, info, gain):
    rows = pieces[0].shape[1]

    def kernel(info_ref, mine_ref, theirs_ref, gain_ref, out_ref):
        write_normed(info_ref, [mine_ref, theirs_ref], gain_ref, out_ref, rows)

    return pl.pallas_call(
        kernel,
        out_shape=jax.ShapeDtypeStruct((rows, D), jnp.bfloat16),
        in_specs=[pl.BlockSpec(memory_space=pltpu.SMEM)] + [pl.BlockSpec(memory_space=VMEM)] * 3,
        out_specs=pl.BlockSpec(memory_space=VMEM),
        compiler_params=pltpu.CompilerParams(vmem_limit_bytes=16 * 1024 * 1024),
        cost_estimate=pl.CostEstimate(
            flops=200 * rows * D, bytes_accessed=4 * rows * D, transcendentals=0
        ),
        name="normalize",
    )(info, *pieces, gain)


def project_pool(xs, info, gain, docs, weights, limit):
    n_x = len(xs)
    n_w = len(weights)
    rows = docs.shape[0]
    scratch = [
        VMEM((SIDE, SIDE, IN_ROWS, BLOCK), jnp.bfloat16),
        VMEM((rows, BLOCK), jnp.float32),
        pltpu.SemaphoreType.DMA((2, n_w)),
    ]
    if n_x > 1:
        scratch.append(VMEM((rows, D), jnp.bfloat16))

    def kernel(*refs):
        info_ref = refs[0]
        x_refs = refs[1 : 1 + n_x]
        gain_ref, docs_ref = refs[1 + n_x : 3 + n_x]
        w_refs = refs[3 + n_x : 3 + n_x + n_w]
        out_ref, m_ref, w_all, acc, sems = refs[3 + n_x + n_w : 8 + n_x + n_w]
        copies = fetch(info_ref, w_refs, 0, IN_ROWS, w_all, sems.at[0])
        m_copies = fetch(info_ref, w_refs, IN_ROWS, MIX_ROWS, m_ref, sems.at[1])
        if n_x > 1:
            normed = refs[-1]
            write_normed(info_ref, x_refs, gain_ref, normed, rows)
        else:
            normed = x_refs[0]
        for c in copies:
            c.wait()
        for n in range(2):
            lanes = pl.ds(n * 256, 256)
            total = None
            for k in range(8):
                part = jnp.dot(
                    normed[:, k * BLOCK : (k + 1) * BLOCK],
                    w_all[k, :, :, lanes].reshape(BLOCK, 256),
                    preferred_element_type=jnp.float32,
                )
                total = part if total is None else total + part
            acc[:, lanes] = total
        own = docs_ref[...]
        masks, count = [], jnp.ones_like(own)
        for j in range(4):
            taken = (pltpu.roll(own, 2**j, 0) == own) & (2**j < info_ref[WINDOW])
            masks.append(taken)
            count = count + jnp.where(taken, pltpu.roll(count, 2**j, 0), 0.0)
        share = 1.0 / count
        for c in range(BLOCK // 128):
            lanes = pl.ds(c * 128, 128)
            proj = acc[:, lanes].astype(jnp.bfloat16).astype(jnp.float32)
            total = proj
            for j in range(4):
                total = total + jnp.where(masks[j], pltpu.roll(total, 2**j, 0), 0.0)
            pooled = total * share - proj
            out_ref[:, lanes] = pooled[WIN:].astype(jnp.bfloat16)
        for c in m_copies:
            c.wait()

    return pl.pallas_call(
        kernel,
        out_shape=[
            jax.ShapeDtypeStruct((rows - WIN, BLOCK), jnp.bfloat16),
            jax.ShapeDtypeStruct((SIDE, SIDE, MIX_ROWS, BLOCK), jnp.bfloat16),
        ],
        in_specs=[pl.BlockSpec(memory_space=pltpu.SMEM)]
        + [pl.BlockSpec(memory_space=VMEM)] * (n_x + 2)
        + [pl.BlockSpec(memory_space=pltpu.HBM)] * n_w,
        out_specs=[pl.BlockSpec(memory_space=VMEM)] * 2,
        scratch_shapes=scratch,
        compiler_params=pltpu.CompilerParams(vmem_limit_bytes=limit * 1024 * 1024),
        cost_estimate=pl.CostEstimate(
            flops=2 * rows * D * BLOCK, bytes_accessed=7 * 1024 * 1024, transcendentals=0
        ),
        name="project_pool",
    )(info, *xs, gain, docs, *weights)


def mix(own, other, info, scale_row, weights):
    rows = own.shape[0]

    def kernel(info_ref, own_ref, other_ref, scale_ref, w_ref, out_ref):
        side = info_ref[SIDE_OF]
        w_own = w_ref[pl.ds(4 * side, 4)].reshape(BLOCK, BLOCK)
        w_other = w_ref[pl.ds(4 * (1 - side), 4)].reshape(BLOCK, BLOCK)
        total = jnp.dot(own_ref[...], w_own, preferred_element_type=jnp.float32)
        total = total + jnp.dot(other_ref[...], w_other, preferred_element_type=jnp.float32)
        out_ref[...] = (total * scale_ref[...]).astype(jnp.bfloat16)

    return pl.pallas_call(
        kernel,
        out_shape=jax.ShapeDtypeStruct((rows, BLOCK), jnp.bfloat16),
        in_specs=[pl.BlockSpec(memory_space=pltpu.SMEM)] + [pl.BlockSpec(memory_space=VMEM)] * 4,
        out_specs=pl.BlockSpec(memory_space=VMEM),
        compiler_params=pltpu.CompilerParams(vmem_limit_bytes=16 * 1024 * 1024),
        cost_estimate=pl.CostEstimate(
            flops=4 * rows * BLOCK * BLOCK, bytes_accessed=2 * 1024 * 1024, transcendentals=0
        ),
        name="mix",
    )(info, own, other, scale_row, weights)


def all_channels(x):
    arrived = [x]
    for k in (1, 2, 3):
        arrived.append(lax.ppermute(x, "tp", tp_perm(lambda t, k=k: t - 2 * k)))
    mine = jnp.stack(arrived, axis=0)
    theirs = lax.ppermute(mine, "tp", tp_perm(lambda t: t ^ 1))
    return [mine, theirs]


def ring(own):
    up, down = [own], [own]
    for _ in range(3):
        above = lax.ppermute(up[-1], ("sp", "tp"), long_shift(1))
        below = lax.ppermute(down[-1], ("sp", "tp"), long_shift(-1))
        above, below = lax.optimization_barrier((above, below))
        up.append(above)
        down.append(below)
    up.append(lax.ppermute(up[-1], ("sp", "tp"), long_shift(1)))
    return up + down[:0:-1]


def shards(tokens, doc_ids, norm_gain, in_proj, mix_proj, out_scale):
    rows = tokens.shape[0]
    tp = lax.axis_index("tp")
    sp = lax.axis_index("sp")
    chip, core = tp // 2, tp % 2
    both_axes = ("sp", "tp")

    w0 = jnp.concatenate([in_proj[0], mix_proj[0]], axis=0)
    w0 = jnp.broadcast_to(w0, (SIDE, BOTH, BLOCK))
    w0 = lax.all_to_all(
        w0, both_axes, split_axis=0, concat_axis=0, tiled=True, axis_index_groups=short_groups()
    )

    w1 = jnp.concatenate([in_proj[1], mix_proj[1]], axis=0)
    w0, w1 = lax.optimization_barrier((w0, w1))
    w1 = lax.all_gather(w1, "sp", axis=0, tiled=True).reshape(SIDE, SIDE, BOTH, BLOCK)
    w0 = ring(w0)

    halo = 2 * WIN
    flags = (doc_ids + 1).astype(jnp.bfloat16)
    flag_row = jnp.pad(flags[rows - halo :], (0, BLOCK - halo)).reshape(1, BLOCK)
    tail = jnp.concatenate([tokens[rows - halo :], jnp.pad(flag_row, ((0, 15), (0, 0)))], axis=0)
    route = [(i, i + 1) for i in range(SIDE * SIDE - 1)]
    tail = lax.ppermute(tail, "sp", route)
    ext_tokens = jnp.concatenate([tail[:halo], tokens], axis=0)
    docs = jnp.concatenate([tail[halo, :halo], flags], axis=0).astype(jnp.float32)
    docs = jnp.broadcast_to(docs[:, None], (rows + halo, 128))

    gain = norm_gain.reshape(2, 8, BLOCK)
    hops = (jnp.arange(4, dtype=jnp.int32) + chip) % 4

    order = jnp.concatenate([2 * hops + core, 2 * hops + 1 - core])
    window = jnp.left_shift(jnp.int32(2), tp % 4)
    place = jnp.where(core == 0, sp // SIDE, sp % SIDE)
    layout = [core, place, tp // 4, window]
    info = jnp.concatenate([order, jnp.stack([v.astype(jnp.int32) for v in layout])])
    scale = lax.dynamic_slice(out_scale, (0, tp * BLOCK), (2, BLOCK))
    partner = tp_perm(lambda t: t ^ 4)

    normed = normalize(all_channels(ext_tokens), info, gain[0])
    pooled, mix_rows = project_pool([normed], info, gain[0], docs, w0, 24)
    other = lax.ppermute(pooled, "tp", partner)
    current = mix(pooled, other, info, scale[0:1], mix_rows)

    pooled, mix_rows = project_pool(all_channels(current), info, gain[1], docs[WIN:], [w1], 50)
    other = lax.ppermute(pooled, "tp", partner)
    return mix(pooled, other, info, scale[1:2], mix_rows)


def solution(mesh):
    placed = (P("sp", "tp"), P("sp"), P(), P(None, "sp", "tp"), P(None, "sp", "tp"), P())
    return jax.shard_map(
        shards, mesh=mesh, in_specs=placed, out_specs=P("sp", "tp"), check_vma=False
    )
```

```python
import jax
import jax.numpy as jnp
from jax import lax
from jax.experimental import pallas as pl
from jax.experimental.pallas import tpu as pltpu
from jax.sharding import PartitionSpec as P


D = 4096
WIN = 16
BLOCK = 512
SIDE = 8
IN_ROWS = 64
MIX_ROWS = 16
BOTH = IN_ROWS + MIX_ROWS
EPS = 1e-06

VMEM = pltpu.VMEM


def device(z, y, t):
    return ((z % SIDE) * SIDE + y % SIDE) * 8 + t


def groups(core_along_y):
    return [
        [device(a, b, t) if t % 2 == core_along_y else device(b, a, t) for b in range(SIDE)]
        for t in range(8)
        for a in range(SIDE)
    ]


def tp_perm(fn):
    return [(t, fn(t) % 8) for t in range(8)]


CORE, SIDE_OF, WINDOW = 8, 9, 10


def fetch(info_ref, gathered, lo, rows, dest, sems):
    along_z, along_y = [], []
    for k in range(SIDE):
        src = gathered.at[k, :, pl.ds(lo, rows), :]
        along_z.append(pltpu.make_async_copy(src, dest.at[k], sems.at[k]))
        along_y.append(pltpu.make_async_copy(src, dest.at[:, k], sems.at[k]))

    @pl.when(info_ref[CORE] == 0)
    def _():
        for c in along_z:
            c.start()

    @pl.when(info_ref[CORE] == 1)
    def _():
        for c in along_y:
            c.start()

    return along_z


def write_normed(info_ref, x_refs, gain_ref, dest, rows):
    def chunk(r, carry):
        here = pl.ds(pl.multiple_of(r * 16, 16), 16)
        values = [x_ref[i, here, :].astype(jnp.float32) for x_ref in x_refs for i in range(4)]
        total = values[0] * values[0]
        for v in values[1:]:
            total = total + v * v
        mean = jnp.sum(total, axis=1, keepdims=True) * (1.0 / D)
        scale = lax.rsqrt(mean + EPS)
        for i, v in enumerate(values):
            block = info_ref[i]
            normed = (v * scale) * gain_ref[pl.ds(block, 1), :]
            lanes = pl.ds(pl.multiple_of(block * BLOCK, BLOCK), BLOCK)
            dest[here, lanes] = normed.astype(jnp.bfloat16)
        return carry

    lax.fori_loop(0, rows // 16, chunk, 0)


def normalize(pieces, info, gain):
    rows = pieces[0].shape[1]

    def kernel(info_ref, mine_ref, theirs_ref, gain_ref, out_ref):
        write_normed(info_ref, [mine_ref, theirs_ref], gain_ref, out_ref, rows)

    return pl.pallas_call(
        kernel,
        out_shape=jax.ShapeDtypeStruct((rows, D), jnp.bfloat16),
        in_specs=[pl.BlockSpec(memory_space=pltpu.SMEM)] + [pl.BlockSpec(memory_space=VMEM)] * 3,
        out_specs=pl.BlockSpec(memory_space=VMEM),
        compiler_params=pltpu.CompilerParams(vmem_limit_bytes=16 * 1024 * 1024),
        cost_estimate=pl.CostEstimate(
            flops=200 * rows * D, bytes_accessed=4 * rows * D, transcendentals=0
        ),
        name="normalize",
    )(info, *pieces, gain)


def project_pool(xs, info, gain, docs, weights, limit):
    n_x = len(xs)
    n_w = 1
    rows = docs.shape[0]
    scratch = [
        VMEM((SIDE, SIDE, IN_ROWS, BLOCK), jnp.bfloat16),
        VMEM((rows, BLOCK), jnp.float32),
        pltpu.SemaphoreType.DMA((2, SIDE)),
    ]
    if n_x > 1:
        scratch.append(VMEM((rows, D), jnp.bfloat16))

    def kernel(*refs):
        info_ref = refs[0]
        x_refs = refs[1 : 1 + n_x]
        gain_ref, docs_ref = refs[1 + n_x : 3 + n_x]
        w_refs = refs[3 + n_x : 3 + n_x + n_w]
        out_ref, m_ref, w_all, acc, sems = refs[3 + n_x + n_w : 8 + n_x + n_w]
        copies = fetch(info_ref, w_refs[0], 0, IN_ROWS, w_all, sems.at[0])
        m_copies = fetch(info_ref, w_refs[0], IN_ROWS, MIX_ROWS, m_ref, sems.at[1])
        if n_x > 1:
            normed = refs[-1]
            write_normed(info_ref, x_refs, gain_ref, normed, rows)
        else:
            normed = x_refs[0]
        for c in copies:
            c.wait()
        for n in range(2):
            lanes = pl.ds(n * 256, 256)
            total = None
            for k in range(8):
                part = jnp.dot(
                    normed[:, k * BLOCK : (k + 1) * BLOCK],
                    w_all[k, :, :, lanes].reshape(BLOCK, 256),
                    preferred_element_type=jnp.float32,
                )
                total = part if total is None else total + part
            acc[:, lanes] = total
        own = docs_ref[...]
        masks, count = [], jnp.ones_like(own)
        for j in range(4):
            taken = (pltpu.roll(own, 2**j, 0) == own) & (2**j < info_ref[WINDOW])
            masks.append(taken)
            count = count + jnp.where(taken, pltpu.roll(count, 2**j, 0), 0.0)
        share = 1.0 / count
        for c in range(BLOCK // 128):
            lanes = pl.ds(c * 128, 128)
            proj = acc[:, lanes].astype(jnp.bfloat16).astype(jnp.float32)
            total = proj
            for j in range(4):
                total = total + jnp.where(masks[j], pltpu.roll(total, 2**j, 0), 0.0)
            pooled = total * share - proj
            out_ref[:, lanes] = pooled[WIN:].astype(jnp.bfloat16)
        for c in m_copies:
            c.wait()

    return pl.pallas_call(
        kernel,
        out_shape=[
            jax.ShapeDtypeStruct((rows - WIN, BLOCK), jnp.bfloat16),
            jax.ShapeDtypeStruct((SIDE, SIDE, MIX_ROWS, BLOCK), jnp.bfloat16),
        ],
        in_specs=[pl.BlockSpec(memory_space=pltpu.SMEM)]
        + [pl.BlockSpec(memory_space=VMEM)] * (n_x + 2)
        + [pl.BlockSpec(memory_space=pltpu.HBM)] * n_w,
        out_specs=[pl.BlockSpec(memory_space=VMEM)] * 2,
        scratch_shapes=scratch,
        compiler_params=pltpu.CompilerParams(vmem_limit_bytes=limit * 1024 * 1024),
        cost_estimate=pl.CostEstimate(
            flops=2 * rows * D * BLOCK, bytes_accessed=7 * 1024 * 1024, transcendentals=0
        ),
        name="project_pool",
    )(info, *xs, gain, docs, weights)


def mix(own, other, info, scale_row, weights):
    rows = own.shape[0]

    def kernel(info_ref, own_ref, other_ref, scale_ref, w_ref, out_ref):
        side = info_ref[SIDE_OF]
        w_own = w_ref[pl.ds(4 * side, 4)].reshape(BLOCK, BLOCK)
        w_other = w_ref[pl.ds(4 * (1 - side), 4)].reshape(BLOCK, BLOCK)
        total = jnp.dot(own_ref[...], w_own, preferred_element_type=jnp.float32)
        total = total + jnp.dot(other_ref[...], w_other, preferred_element_type=jnp.float32)
        out_ref[...] = (total * scale_ref[...]).astype(jnp.bfloat16)

    return pl.pallas_call(
        kernel,
        out_shape=jax.ShapeDtypeStruct((rows, BLOCK), jnp.bfloat16),
        in_specs=[pl.BlockSpec(memory_space=pltpu.SMEM)] + [pl.BlockSpec(memory_space=VMEM)] * 4,
        out_specs=pl.BlockSpec(memory_space=VMEM),
        compiler_params=pltpu.CompilerParams(vmem_limit_bytes=16 * 1024 * 1024),
        cost_estimate=pl.CostEstimate(
            flops=4 * rows * BLOCK * BLOCK, bytes_accessed=2 * 1024 * 1024, transcendentals=0
        ),
        name="mix",
    )(info, own, other, scale_row, weights)


def all_channels(x):
    arrived = [x]
    for k in (1, 2, 3):
        arrived.append(lax.ppermute(x, "tp", tp_perm(lambda t, k=k: t - 2 * k)))
    mine = jnp.stack(arrived, axis=0)
    theirs = lax.ppermute(mine, "tp", tp_perm(lambda t: t ^ 1))
    return [mine, theirs]


def gather_weights(in_rows, mix_rows):
    own = jnp.concatenate([in_rows, mix_rows], axis=0)
    own = jnp.broadcast_to(own, (SIDE, BOTH, BLOCK))
    own = lax.all_to_all(
        own, ("sp", "tp"), split_axis=0, concat_axis=0, tiled=True, axis_index_groups=groups(0)
    )
    own = own.reshape(SIDE * BOTH, BLOCK)
    own = lax.all_gather(own, ("sp", "tp"), axis=0, tiled=True, axis_index_groups=groups(1))
    return own.reshape(SIDE, SIDE, BOTH, BLOCK)


def shards(tokens, doc_ids, norm_gain, in_proj, mix_proj, out_scale):
    rows = tokens.shape[0]
    tp = lax.axis_index("tp")
    chip, core = tp // 2, tp % 2
    w0 = gather_weights(in_proj[0], mix_proj[0])
    w1 = gather_weights(in_proj[1], mix_proj[1])

    halo = 2 * WIN
    flags = (doc_ids + 1).astype(jnp.bfloat16)
    flag_row = jnp.pad(flags[rows - halo :], (0, BLOCK - halo)).reshape(1, BLOCK)
    tail = jnp.concatenate([tokens[rows - halo :], jnp.pad(flag_row, ((0, 15), (0, 0)))], axis=0)
    route = [(i, i + 1) for i in range(SIDE * SIDE - 1)]
    tail = lax.ppermute(tail, "sp", route)
    ext_tokens = jnp.concatenate([tail[:halo], tokens], axis=0)
    docs = jnp.concatenate([tail[halo, :halo], flags], axis=0).astype(jnp.float32)
    docs = jnp.broadcast_to(docs[:, None], (rows + halo, 128))

    gain = norm_gain.reshape(2, 8, BLOCK)
    hops = (jnp.arange(4, dtype=jnp.int32) + chip) % 4

    order = jnp.concatenate([2 * hops + core, 2 * hops + 1 - core])
    window = jnp.left_shift(jnp.int32(2), tp % 4)
    layout = [core, tp // 4, window]
    info = jnp.concatenate([order, jnp.stack([v.astype(jnp.int32) for v in layout])])
    scale = lax.dynamic_slice(out_scale, (0, tp * BLOCK), (2, BLOCK))
    partner = tp_perm(lambda t: t ^ 4)

    normed = normalize(all_channels(ext_tokens), info, gain[0])
    pooled, mix_rows = project_pool([normed], info, gain[0], docs, w0, 50)
    other = lax.ppermute(pooled, "tp", partner)
    current = mix(pooled, other, info, scale[0:1], mix_rows)

    pooled, mix_rows = project_pool(all_channels(current), info, gain[1], docs[WIN:], w1, 50)
    other = lax.ppermute(pooled, "tp", partner)
    return mix(pooled, other, info, scale[1:2], mix_rows)


def solution(mesh):
    placed = (P("sp", "tp"), P("sp"), P(), P(None, "sp", "tp"), P(None, "sp", "tp"), P())
    return jax.shard_map(
        shards, mesh=mesh, in_specs=placed, out_specs=P("sp", "tp"), check_vma=False
    )
```

```python
import jax
import jax.numpy as jnp
from jax import lax
from jax.experimental import pallas as pl
from jax.experimental.pallas import tpu as pltpu
from jax.sharding import PartitionSpec as P


D = 4096
WIN = 16
BLOCK = 512
SIDE = 8
IN_ROWS = 64
MIX_ROWS = 16
BOTH = IN_ROWS + MIX_ROWS
EPS = 1e-06

VMEM = pltpu.VMEM


def device(z, y, t):
    return ((z % SIDE) * SIDE + y % SIDE) * 8 + t


def groups(core_along_y):
    return [
        [device(a, b, t) if t % 2 == core_along_y else device(b, a, t) for b in range(SIDE)]
        for t in range(8)
        for a in range(SIDE)
    ]


def tp_perm(fn):
    return [(t, fn(t) % 8) for t in range(8)]


CORE, SIDE_OF, WINDOW = 8, 9, 10


def fetch(info_ref, gathered, lo, rows, dest, sems):
    along_z, along_y = [], []
    for z in range(SIDE):
        along_z.append(
            pltpu.make_async_copy(gathered.at[z, :, pl.ds(lo, rows), :], dest.at[z], sems.at[z])
        )
        along_y.append(
            pltpu.make_async_copy(gathered.at[:, z, pl.ds(lo, rows), :], dest.at[z], sems.at[z])
        )

    @pl.when(info_ref[CORE] == 0)
    def _():
        for c in along_z:
            c.start()

    @pl.when(info_ref[CORE] == 1)
    def _():
        for c in along_y:
            c.start()

    return along_z


def write_normed(info_ref, x_refs, gain_ref, dest, rows):
    def chunk(r, carry):
        here = pl.ds(pl.multiple_of(r * 16, 16), 16)
        values = [x_ref[i, here, :].astype(jnp.float32) for x_ref in x_refs for i in range(4)]
        total = values[0] * values[0]
        for v in values[1:]:
            total = total + v * v
        mean = jnp.sum(total, axis=1, keepdims=True) * (1.0 / D)
        scale = lax.rsqrt(mean + EPS)
        for i, v in enumerate(values):
            block = info_ref[i]
            normed = (v * scale) * gain_ref[pl.ds(block, 1), :]
            lanes = pl.ds(pl.multiple_of(block * BLOCK, BLOCK), BLOCK)
            dest[here, lanes] = normed.astype(jnp.bfloat16)
        return carry

    lax.fori_loop(0, rows // 16, chunk, 0)


def normalize(pieces, info, gain):
    rows = pieces[0].shape[1]

    def kernel(info_ref, mine_ref, theirs_ref, gain_ref, out_ref):
        write_normed(info_ref, [mine_ref, theirs_ref], gain_ref, out_ref, rows)

    return pl.pallas_call(
        kernel,
        out_shape=jax.ShapeDtypeStruct((rows, D), jnp.bfloat16),
        in_specs=[pl.BlockSpec(memory_space=pltpu.SMEM)] + [pl.BlockSpec(memory_space=VMEM)] * 3,
        out_specs=pl.BlockSpec(memory_space=VMEM),
        compiler_params=pltpu.CompilerParams(vmem_limit_bytes=16 * 1024 * 1024),
        cost_estimate=pl.CostEstimate(
            flops=200 * rows * D, bytes_accessed=4 * rows * D, transcendentals=0
        ),
        name="normalize",
    )(info, *pieces, gain)


def project_pool(xs, info, gain, docs, weights, limit):
    n_x = len(xs)
    n_w = 1
    rows = docs.shape[0]
    scratch = [
        VMEM((SIDE, SIDE, IN_ROWS, BLOCK), jnp.bfloat16),
        VMEM((rows, BLOCK), jnp.float32),
        pltpu.SemaphoreType.DMA((2, SIDE)),
    ]
    if n_x > 1:
        scratch.append(VMEM((rows, D), jnp.bfloat16))

    def kernel(*refs):
        info_ref = refs[0]
        x_refs = refs[1 : 1 + n_x]
        gain_ref, docs_ref = refs[1 + n_x : 3 + n_x]
        w_refs = refs[3 + n_x : 3 + n_x + n_w]
        out_ref, m_ref, w_all, acc, sems = refs[3 + n_x + n_w : 8 + n_x + n_w]
        copies = fetch(info_ref, w_refs[0], 0, IN_ROWS, w_all, sems.at[0])
        m_copies = fetch(info_ref, w_refs[0], IN_ROWS, MIX_ROWS, m_ref, sems.at[1])
        if n_x > 1:
            normed = refs[-1]
            write_normed(info_ref, x_refs, gain_ref, normed, rows)
        else:
            normed = x_refs[0]
        for z, c in enumerate(copies):
            c.wait()
            part = jnp.dot(
                normed[:, z * BLOCK : (z + 1) * BLOCK],
                w_all[z].reshape(BLOCK, BLOCK),
                preferred_element_type=jnp.float32,
            )
            acc[...] = part if z == 0 else acc[...] + part
        own = docs_ref[...]
        masks, count = [], jnp.ones_like(own)
        for j in range(4):
            taken = (pltpu.roll(own, 2**j, 0) == own) & (2**j < info_ref[WINDOW])
            masks.append(taken)
            count = count + jnp.where(taken, pltpu.roll(count, 2**j, 0), 0.0)
        share = 1.0 / count
        for c in range(BLOCK // 128):
            lanes = pl.ds(c * 128, 128)
            proj = acc[:, lanes].astype(jnp.bfloat16).astype(jnp.float32)
            total = proj
            for j in range(4):
                total = total + jnp.where(masks[j], pltpu.roll(total, 2**j, 0), 0.0)
            pooled = total * share - proj
            out_ref[:, lanes] = pooled[WIN:].astype(jnp.bfloat16)
        for c in m_copies:
            c.wait()

    return pl.pallas_call(
        kernel,
        out_shape=[
            jax.ShapeDtypeStruct((rows - WIN, BLOCK), jnp.bfloat16),
            jax.ShapeDtypeStruct((SIDE, SIDE, MIX_ROWS, BLOCK), jnp.bfloat16),
        ],
        in_specs=[pl.BlockSpec(memory_space=pltpu.SMEM)]
        + [pl.BlockSpec(memory_space=VMEM)] * (n_x + 2)
        + [pl.BlockSpec(memory_space=pltpu.HBM)] * n_w,
        out_specs=[pl.BlockSpec(memory_space=VMEM)] * 2,
        scratch_shapes=scratch,
        compiler_params=pltpu.CompilerParams(vmem_limit_bytes=limit * 1024 * 1024),
        cost_estimate=pl.CostEstimate(
            flops=2 * rows * D * BLOCK, bytes_accessed=7 * 1024 * 1024, transcendentals=0
        ),
        name="project_pool",
    )(info, *xs, gain, docs, weights)


def mix(own, other, info, scale_row, weights):
    rows = own.shape[0]

    def kernel(info_ref, own_ref, other_ref, scale_ref, w_ref, out_ref):
        side = info_ref[SIDE_OF]
        w_own = w_ref[pl.ds(4 * side, 4)].reshape(BLOCK, BLOCK)
        w_other = w_ref[pl.ds(4 * (1 - side), 4)].reshape(BLOCK, BLOCK)
        total = jnp.dot(own_ref[...], w_own, preferred_element_type=jnp.float32)
        total = total + jnp.dot(other_ref[...], w_other, preferred_element_type=jnp.float32)
        out_ref[...] = (total * scale_ref[...]).astype(jnp.bfloat16)

    return pl.pallas_call(
        kernel,
        out_shape=jax.ShapeDtypeStruct((rows, BLOCK), jnp.bfloat16),
        in_specs=[pl.BlockSpec(memory_space=pltpu.SMEM)] + [pl.BlockSpec(memory_space=VMEM)] * 4,
        out_specs=pl.BlockSpec(memory_space=VMEM),
        compiler_params=pltpu.CompilerParams(vmem_limit_bytes=16 * 1024 * 1024),
        cost_estimate=pl.CostEstimate(
            flops=4 * rows * BLOCK * BLOCK, bytes_accessed=2 * 1024 * 1024, transcendentals=0
        ),
        name="mix",
    )(info, own, other, scale_row, weights)


def all_channels(x):
    arrived = [x]
    for k in (1, 2, 3):
        arrived.append(lax.ppermute(x, "tp", tp_perm(lambda t, k=k: t - 2 * k)))
    mine = jnp.stack(arrived, axis=0)
    theirs = lax.ppermute(mine, "tp", tp_perm(lambda t: t ^ 1))
    return [mine, theirs]


def eight_copies(in_proj, mix_proj):
    def kernel(in_ref, mix_ref, out_ref):
        for layer in range(2):
            for i in range(SIDE):
                out_ref[i, layer * BOTH : layer * BOTH + IN_ROWS] = in_ref[layer]
                out_ref[i, layer * BOTH + IN_ROWS : (layer + 1) * BOTH] = mix_ref[layer]

    return pl.pallas_call(
        kernel,
        out_shape=jax.ShapeDtypeStruct((SIDE, 2 * BOTH, BLOCK), jnp.bfloat16),
        in_specs=[pl.BlockSpec(memory_space=VMEM)] * 2,
        out_specs=pl.BlockSpec(memory_space=VMEM),
        name="eight_copies",
    )(in_proj, mix_proj)


def gather_weights(in_proj, mix_proj):
    own = eight_copies(in_proj, mix_proj)
    own = lax.all_to_all(
        own, ("sp", "tp"), split_axis=0, concat_axis=0, tiled=True, axis_index_groups=groups(0)
    )
    gathered = []
    for layer in range(2):
        rows = own[:, layer * BOTH : (layer + 1) * BOTH].reshape(SIDE * BOTH, BLOCK)
        rows = lax.all_gather(rows, ("sp", "tp"), axis=0, tiled=True, axis_index_groups=groups(1))
        gathered.append(rows.reshape(SIDE, SIDE, BOTH, BLOCK))
    return gathered


def shards(tokens, doc_ids, norm_gain, in_proj, mix_proj, out_scale):
    rows = tokens.shape[0]
    tp = lax.axis_index("tp")
    chip, core = tp // 2, tp % 2
    w0, w1 = gather_weights(in_proj, mix_proj)

    halo = 2 * WIN
    flags = (doc_ids + 1).astype(jnp.bfloat16)
    flag_row = jnp.pad(flags[rows - halo :], (0, BLOCK - halo)).reshape(1, BLOCK)
    tail = jnp.concatenate([tokens[rows - halo :], jnp.pad(flag_row, ((0, 15), (0, 0)))], axis=0)
    route = [(i, i + 1) for i in range(SIDE * SIDE - 1)]
    tail = lax.ppermute(tail, "sp", route)
    ext_tokens = jnp.concatenate([tail[:halo], tokens], axis=0)
    docs = jnp.concatenate([tail[halo, :halo], flags], axis=0).astype(jnp.float32)
    docs = jnp.broadcast_to(docs[:, None], (rows + halo, 128))

    gain = norm_gain.reshape(2, 8, BLOCK)
    hops = (jnp.arange(4, dtype=jnp.int32) + chip) % 4

    order = jnp.concatenate([2 * hops + core, 2 * hops + 1 - core])
    window = jnp.left_shift(jnp.int32(2), tp % 4)
    layout = [core, tp // 4, window]
    info = jnp.concatenate([order, jnp.stack([v.astype(jnp.int32) for v in layout])])
    scale = lax.dynamic_slice(out_scale, (0, tp * BLOCK), (2, BLOCK))
    partner = tp_perm(lambda t: t ^ 4)

    normed = normalize(all_channels(ext_tokens), info, gain[0])
    pooled, mix_rows = project_pool([normed], info, gain[0], docs, w0, 48)
    other = lax.ppermute(pooled, "tp", partner)
    current = mix(pooled, other, info, scale[0:1], mix_rows)

    pooled, mix_rows = project_pool(all_channels(current), info, gain[1], docs[WIN:], w1, 50)
    other = lax.ppermute(pooled, "tp", partner)
    return mix(pooled, other, info, scale[1:2], mix_rows)


def solution(mesh):
    placed = (P("sp", "tp"), P("sp"), P(), P(None, "sp", "tp"), P(None, "sp", "tp"), P())
    return jax.shard_map(
        shards, mesh=mesh, in_specs=placed, out_specs=P("sp", "tp"), check_vma=False
    )
```

```python
import jax
import jax.numpy as jnp
from jax import lax
from jax.experimental import pallas as pl
from jax.experimental.pallas import tpu as pltpu
from jax.sharding import PartitionSpec as P


D = 4096
WIN = 16
BLOCK = 512
SIDE = 8
IN_ROWS = 64
MIX_ROWS = 16
BOTH = IN_ROWS + MIX_ROWS
EPS = 1e-06

VMEM = pltpu.VMEM


def device(z, y, t):
    return ((z % SIDE) * SIDE + y % SIDE) * 8 + t


def groups(core_along_y):
    return [
        [device(a, b, t) if t % 2 == core_along_y else device(b, a, t) for b in range(SIDE)]
        for t in range(8)
        for a in range(SIDE)
    ]


def tp_perm(fn):
    return [(t, fn(t) % 8) for t in range(8)]


CORE, SIDE_OF, WINDOW = 8, 9, 10


def fetch(info_ref, gathered, lo, rows, dest, sems):
    along_z, along_y = [], []
    for z in range(SIDE):
        along_z.append(
            pltpu.make_async_copy(gathered.at[z, :, pl.ds(lo, rows), :], dest.at[z], sems.at[z])
        )
        along_y.append(
            pltpu.make_async_copy(gathered.at[:, z, pl.ds(lo, rows), :], dest.at[z], sems.at[z])
        )

    @pl.when(info_ref[CORE] == 0)
    def _():
        for c in along_z:
            c.start()

    @pl.when(info_ref[CORE] == 1)
    def _():
        for c in along_y:
            c.start()

    return along_z


def write_normed(info_ref, x_refs, gain_ref, dest, rows):
    def chunk(r, carry):
        here = pl.ds(pl.multiple_of(r * 16, 16), 16)
        values = [x_ref[i, here, :].astype(jnp.float32) for x_ref in x_refs for i in range(4)]
        total = values[0] * values[0]
        for v in values[1:]:
            total = total + v * v
        mean = jnp.sum(total, axis=1, keepdims=True) * (1.0 / D)
        scale = lax.rsqrt(mean + EPS)
        for i, v in enumerate(values):
            block = info_ref[i]
            normed = (v * scale) * gain_ref[pl.ds(block, 1), :]
            lanes = pl.ds(pl.multiple_of(block * BLOCK, BLOCK), BLOCK)
            dest[here, lanes] = normed.astype(jnp.bfloat16)
        return carry

    lax.fori_loop(0, rows // 16, chunk, 0)


def normalize(pieces, info, gain):
    rows = pieces[0].shape[1]

    def kernel(info_ref, mine_ref, theirs_ref, gain_ref, out_ref):
        write_normed(info_ref, [mine_ref, theirs_ref], gain_ref, out_ref, rows)

    return pl.pallas_call(
        kernel,
        out_shape=jax.ShapeDtypeStruct((rows, D), jnp.bfloat16),
        in_specs=[pl.BlockSpec(memory_space=pltpu.SMEM)] + [pl.BlockSpec(memory_space=VMEM)] * 3,
        out_specs=pl.BlockSpec(memory_space=VMEM),
        compiler_params=pltpu.CompilerParams(vmem_limit_bytes=16 * 1024 * 1024),
        cost_estimate=pl.CostEstimate(
            flops=200 * rows * D, bytes_accessed=4 * rows * D, transcendentals=0
        ),
        name="normalize",
    )(info, *pieces, gain)


def project_pool(normed, info, docs, weights, limit):
    rows = docs.shape[0]

    def kernel(info_ref, normed_ref, docs_ref, w_ref, out_ref, m_ref, w_all, acc, sems):
        copies = fetch(info_ref, w_ref, 0, IN_ROWS, w_all, sems.at[0])
        m_copies = fetch(info_ref, w_ref, IN_ROWS, MIX_ROWS, m_ref, sems.at[1])
        for z, c in enumerate(copies):
            c.wait()
            part = jnp.dot(
                normed_ref[:, z * BLOCK : (z + 1) * BLOCK],
                w_all[z].reshape(BLOCK, BLOCK),
                preferred_element_type=jnp.float32,
            )
            acc[...] = part if z == 0 else acc[...] + part
        own = docs_ref[...]
        masks, count = [], jnp.ones_like(own)
        for j in range(4):
            taken = (pltpu.roll(own, 2**j, 0) == own) & (2**j < info_ref[WINDOW])
            masks.append(taken)
            count = count + jnp.where(taken, pltpu.roll(count, 2**j, 0), 0.0)
        share = 1.0 / count
        for c in range(BLOCK // 128):
            lanes = pl.ds(c * 128, 128)
            proj = acc[:, lanes].astype(jnp.bfloat16).astype(jnp.float32)
            total = proj
            for j in range(4):
                total = total + jnp.where(masks[j], pltpu.roll(total, 2**j, 0), 0.0)
            pooled = total * share - proj
            out_ref[:, lanes] = pooled[WIN:].astype(jnp.bfloat16)
        for c in m_copies:
            c.wait()

    return pl.pallas_call(
        kernel,
        out_shape=[
            jax.ShapeDtypeStruct((rows - WIN, BLOCK), jnp.bfloat16),
            jax.ShapeDtypeStruct((SIDE, SIDE, MIX_ROWS, BLOCK), jnp.bfloat16),
        ],
        in_specs=[pl.BlockSpec(memory_space=pltpu.SMEM)]
        + [pl.BlockSpec(memory_space=VMEM)] * 2
        + [pl.BlockSpec(memory_space=pltpu.HBM)],
        out_specs=[pl.BlockSpec(memory_space=VMEM)] * 2,
        scratch_shapes=[
            VMEM((SIDE, SIDE, IN_ROWS, BLOCK), jnp.bfloat16),
            VMEM((rows, BLOCK), jnp.float32),
            pltpu.SemaphoreType.DMA((2, SIDE)),
        ],
        compiler_params=pltpu.CompilerParams(vmem_limit_bytes=limit * 1024 * 1024),
        cost_estimate=pl.CostEstimate(
            flops=2 * rows * D * BLOCK, bytes_accessed=7 * 1024 * 1024, transcendentals=0
        ),
        name="project_pool",
    )(info, normed, docs, weights)


def mix(own, other, info, scale_row, weights):
    rows = own.shape[0]

    def kernel(info_ref, own_ref, other_ref, scale_ref, w_ref, out_ref):
        side = info_ref[SIDE_OF]
        w_own = w_ref[pl.ds(4 * side, 4)].reshape(BLOCK, BLOCK)
        w_other = w_ref[pl.ds(4 * (1 - side), 4)].reshape(BLOCK, BLOCK)
        total = jnp.dot(own_ref[...], w_own, preferred_element_type=jnp.float32)
        total = total + jnp.dot(other_ref[...], w_other, preferred_element_type=jnp.float32)
        out_ref[...] = (total * scale_ref[...]).astype(jnp.bfloat16)

    return pl.pallas_call(
        kernel,
        out_shape=jax.ShapeDtypeStruct((rows, BLOCK), jnp.bfloat16),
        in_specs=[pl.BlockSpec(memory_space=pltpu.SMEM)] + [pl.BlockSpec(memory_space=VMEM)] * 4,
        out_specs=pl.BlockSpec(memory_space=VMEM),
        compiler_params=pltpu.CompilerParams(vmem_limit_bytes=16 * 1024 * 1024),
        cost_estimate=pl.CostEstimate(
            flops=4 * rows * BLOCK * BLOCK, bytes_accessed=2 * 1024 * 1024, transcendentals=0
        ),
        name="mix",
    )(info, own, other, scale_row, weights)


def all_channels(x):
    arrived = [x]
    for k in (1, 2, 3):
        arrived.append(lax.ppermute(x, "tp", tp_perm(lambda t, k=k: t - 2 * k)))
    mine = jnp.stack(arrived, axis=0)
    theirs = lax.ppermute(mine, "tp", tp_perm(lambda t: t ^ 1))
    return [mine, theirs]


def eight_copies(in_proj, mix_proj):
    def kernel(in_ref, mix_ref, out_ref):
        for layer in range(2):
            for i in range(SIDE):
                out_ref[i, layer * BOTH : layer * BOTH + IN_ROWS] = in_ref[layer]
                out_ref[i, layer * BOTH + IN_ROWS : (layer + 1) * BOTH] = mix_ref[layer]

    return pl.pallas_call(
        kernel,
        out_shape=jax.ShapeDtypeStruct((SIDE, 2 * BOTH, BLOCK), jnp.bfloat16),
        in_specs=[pl.BlockSpec(memory_space=VMEM)] * 2,
        out_specs=pl.BlockSpec(memory_space=VMEM),
        name="eight_copies",
    )(in_proj, mix_proj)


def gather_weights(in_proj, mix_proj):
    own = eight_copies(in_proj, mix_proj)
    own = lax.all_to_all(
        own, ("sp", "tp"), split_axis=0, concat_axis=0, tiled=True, axis_index_groups=groups(0)
    )
    gathered = []
    for layer in range(2):
        rows = own[:, layer * BOTH : (layer + 1) * BOTH].reshape(SIDE * BOTH, BLOCK)
        rows = lax.all_gather(rows, ("sp", "tp"), axis=0, tiled=True, axis_index_groups=groups(1))
        gathered.append(rows.reshape(SIDE, SIDE, BOTH, BLOCK))
    return gathered


def shards(tokens, doc_ids, norm_gain, in_proj, mix_proj, out_scale):
    rows = tokens.shape[0]
    tp = lax.axis_index("tp")
    chip, core = tp // 2, tp % 2
    w0, w1 = gather_weights(in_proj, mix_proj)

    halo = 2 * WIN
    flags = (doc_ids + 1).astype(jnp.bfloat16)
    flag_row = jnp.pad(flags[rows - halo :], (0, BLOCK - halo)).reshape(1, BLOCK)
    tail = jnp.concatenate([tokens[rows - halo :], jnp.pad(flag_row, ((0, 15), (0, 0)))], axis=0)
    route = [(i, i + 1) for i in range(SIDE * SIDE - 1)]
    tail = lax.ppermute(tail, "sp", route)
    ext_tokens = jnp.concatenate([tail[:halo], tokens], axis=0)
    docs = jnp.concatenate([tail[halo, :halo], flags], axis=0).astype(jnp.float32)
    docs = jnp.broadcast_to(docs[:, None], (rows + halo, 128))

    gain = norm_gain.reshape(2, 8, BLOCK)
    hops = (jnp.arange(4, dtype=jnp.int32) + chip) % 4

    order = jnp.concatenate([2 * hops + core, 2 * hops + 1 - core])
    window = jnp.left_shift(jnp.int32(2), tp % 4)
    layout = [core, tp // 4, window]
    info = jnp.concatenate([order, jnp.stack([v.astype(jnp.int32) for v in layout])])
    scale = lax.dynamic_slice(out_scale, (0, tp * BLOCK), (2, BLOCK))
    partner = tp_perm(lambda t: t ^ 4)

    normed = normalize(all_channels(ext_tokens), info, gain[0])
    pooled, mix_rows = project_pool(normed, info, docs, w0, 50)
    other = lax.ppermute(pooled, "tp", partner)
    current = mix(pooled, other, info, scale[0:1], mix_rows)

    normed = normalize(all_channels(current), info, gain[1])
    pooled, mix_rows = project_pool(normed, info, docs[WIN:], w1, 48)
    other = lax.ppermute(pooled, "tp", partner)
    return mix(pooled, other, info, scale[1:2], mix_rows)


def solution(mesh):
    placed = (P("sp", "tp"), P("sp"), P(), P(None, "sp", "tp"), P(None, "sp", "tp"), P())
    return jax.shard_map(
        shards, mesh=mesh, in_specs=placed, out_specs=P("sp", "tp"), check_vma=False
    )
```

```python
import jax
import jax.numpy as jnp
from jax import lax
from jax.experimental import pallas as pl
from jax.experimental.pallas import tpu as pltpu
from jax.sharding import PartitionSpec as P


D = 4096
WIN = 16
BLOCK = 512
SIDE = 8
IN_ROWS = 64
MIX_ROWS = 16
BOTH = IN_ROWS + MIX_ROWS
EPS = 1e-06

VMEM = pltpu.VMEM


def device(z, y, t):
    return ((z % SIDE) * SIDE + y % SIDE) * 8 + t


def groups(core_along_y):
    return [
        [device(a, b, t) if t % 2 == core_along_y else device(b, a, t) for b in range(SIDE)]
        for t in range(8)
        for a in range(SIDE)
    ]


def tp_perm(fn):
    return [(t, fn(t) % 8) for t in range(8)]


CORE, SIDE_OF, WINDOW = 8, 9, 10


def fetch(info_ref, gathered, lo, rows, dest, sems):
    along_z, along_y = [], []
    for z in range(SIDE):
        along_z.append(
            pltpu.make_async_copy(gathered.at[z, :, pl.ds(lo, rows), :], dest.at[z], sems.at[z])
        )
        along_y.append(
            pltpu.make_async_copy(gathered.at[:, z, pl.ds(lo, rows), :], dest.at[z], sems.at[z])
        )

    @pl.when(info_ref[CORE] == 0)
    def _():
        for c in along_z:
            c.start()

    @pl.when(info_ref[CORE] == 1)
    def _():
        for c in along_y:
            c.start()

    return along_z


def write_normed(info_ref, x_refs, gain_ref, dest, rows):
    def chunk(r, carry):
        here = pl.ds(pl.multiple_of(r * 16, 16), 16)
        values = [x_ref[i, here, :].astype(jnp.float32) for x_ref in x_refs for i in range(4)]
        total = values[0] * values[0]
        for v in values[1:]:
            total = total + v * v
        mean = jnp.sum(total, axis=1, keepdims=True) * (1.0 / D)
        scale = lax.rsqrt(mean + EPS)
        for i, v in enumerate(values):
            block = info_ref[i]
            normed = (v * scale) * gain_ref[pl.ds(block, 1), :]
            lanes = pl.ds(pl.multiple_of(block * BLOCK, BLOCK), BLOCK)
            dest[here, lanes] = normed.astype(jnp.bfloat16)
        return carry

    lax.fori_loop(0, rows // 16, chunk, 0)


def normalize(pieces, info, gain):
    rows = pieces[0].shape[1]

    def kernel(info_ref, mine_ref, theirs_ref, gain_ref, out_ref):
        write_normed(info_ref, [mine_ref, theirs_ref], gain_ref, out_ref, rows)

    return pl.pallas_call(
        kernel,
        out_shape=jax.ShapeDtypeStruct((rows, D), jnp.bfloat16),
        in_specs=[pl.BlockSpec(memory_space=pltpu.SMEM)] + [pl.BlockSpec(memory_space=VMEM)] * 3,
        out_specs=pl.BlockSpec(memory_space=VMEM),
        compiler_params=pltpu.CompilerParams(vmem_limit_bytes=16 * 1024 * 1024),
        cost_estimate=pl.CostEstimate(
            flops=200 * rows * D, bytes_accessed=4 * rows * D, transcendentals=0
        ),
        name="normalize",
    )(info, *pieces, gain)


def project_pool(normed, info, docs, weights, limit):
    rows = docs.shape[0]

    def kernel(info_ref, normed_ref, docs_ref, w_ref, out_ref, m_ref, w_all, acc, sems):
        copies = fetch(info_ref, w_ref, 0, IN_ROWS, w_all, sems.at[0])
        m_copies = fetch(info_ref, w_ref, IN_ROWS, MIX_ROWS, m_ref, sems.at[1])
        for z, c in enumerate(copies):
            c.wait()
            part = jnp.dot(
                normed_ref[:, z * BLOCK : (z + 1) * BLOCK],
                w_all[z].reshape(BLOCK, BLOCK),
                preferred_element_type=jnp.float32,
            )
            acc[...] = part if z == 0 else acc[...] + part
        own = docs_ref[...]
        masks, count = [], jnp.ones_like(own)
        for j in range(4):
            taken = (pltpu.roll(own, 2**j, 0) == own) & (2**j < info_ref[WINDOW])
            masks.append(taken)
            count = count + jnp.where(taken, pltpu.roll(count, 2**j, 0), 0.0)
        share = 1.0 / count
        for c in range(BLOCK // 128):
            lanes = pl.ds(c * 128, 128)
            proj = acc[:, lanes].astype(jnp.bfloat16).astype(jnp.float32)
            total = proj
            for j in range(4):
                total = total + jnp.where(masks[j], pltpu.roll(total, 2**j, 0), 0.0)
            pooled = total * share - proj
            out_ref[:, lanes] = pooled[WIN:].astype(jnp.bfloat16)
        for c in m_copies:
            c.wait()

    return pl.pallas_call(
        kernel,
        out_shape=[
            jax.ShapeDtypeStruct((rows - WIN, BLOCK), jnp.bfloat16),
            jax.ShapeDtypeStruct((SIDE, SIDE, MIX_ROWS, BLOCK), jnp.bfloat16),
        ],
        in_specs=[
            pl.BlockSpec(memory_space=pltpu.SMEM),
            pl.BlockSpec(memory_space=VMEM),
            pl.BlockSpec(memory_space=VMEM),
            pl.BlockSpec(memory_space=pltpu.HBM),
        ],
        out_specs=[pl.BlockSpec(memory_space=VMEM)] * 2,
        scratch_shapes=[
            VMEM((SIDE, SIDE, IN_ROWS, BLOCK), jnp.bfloat16),
            VMEM((rows, BLOCK), jnp.float32),
            pltpu.SemaphoreType.DMA((2, SIDE)),
        ],
        compiler_params=pltpu.CompilerParams(vmem_limit_bytes=limit * 1024 * 1024),
        cost_estimate=pl.CostEstimate(
            flops=2 * rows * D * BLOCK, bytes_accessed=7 * 1024 * 1024, transcendentals=0
        ),
        name="project_pool",
    )(info, normed, docs, weights)


def mix(own, other, info, scale_row, weights):
    rows = own.shape[0]

    def kernel(info_ref, own_ref, other_ref, scale_ref, w_ref, out_ref):
        side = info_ref[SIDE_OF]
        w_own = w_ref[pl.ds(4 * side, 4)].reshape(BLOCK, BLOCK)
        w_other = w_ref[pl.ds(4 * (1 - side), 4)].reshape(BLOCK, BLOCK)
        total = jnp.dot(own_ref[...], w_own, preferred_element_type=jnp.float32)
        total = total + jnp.dot(other_ref[...], w_other, preferred_element_type=jnp.float32)
        out_ref[...] = (total * scale_ref[...]).astype(jnp.bfloat16)

    return pl.pallas_call(
        kernel,
        out_shape=jax.ShapeDtypeStruct((rows, BLOCK), jnp.bfloat16),
        in_specs=[pl.BlockSpec(memory_space=pltpu.SMEM)] + [pl.BlockSpec(memory_space=VMEM)] * 4,
        out_specs=pl.BlockSpec(memory_space=VMEM),
        compiler_params=pltpu.CompilerParams(vmem_limit_bytes=16 * 1024 * 1024),
        cost_estimate=pl.CostEstimate(
            flops=4 * rows * BLOCK * BLOCK, bytes_accessed=2 * 1024 * 1024, transcendentals=0
        ),
        name="mix",
    )(info, own, other, scale_row, weights)


def all_channels(x):
    arrived = [x]
    for k in (1, 2, 3):
        arrived.append(lax.ppermute(x, "tp", tp_perm(lambda t, k=k: t - 2 * k)))
    mine = jnp.stack(arrived, axis=0)
    theirs = lax.ppermute(mine, "tp", tp_perm(lambda t: t ^ 1))
    return [mine, theirs]


def eight_copies(in_proj, mix_proj):
    def kernel(in_ref, mix_ref, out_ref):
        for layer in range(2):
            for i in range(SIDE):
                out_ref[i, layer * BOTH : layer * BOTH + IN_ROWS] = in_ref[layer]
                out_ref[i, layer * BOTH + IN_ROWS : (layer + 1) * BOTH] = mix_ref[layer]

    return pl.pallas_call(
        kernel,
        out_shape=jax.ShapeDtypeStruct((SIDE, 2 * BOTH, BLOCK), jnp.bfloat16),
        in_specs=[pl.BlockSpec(memory_space=VMEM)] * 2,
        out_specs=pl.BlockSpec(memory_space=VMEM),
        name="eight_copies",
    )(in_proj, mix_proj)


def short_way(in_proj, mix_proj):
    own = eight_copies(in_proj, mix_proj)
    return lax.all_to_all(
        own, ("sp", "tp"), split_axis=0, concat_axis=0, tiled=True, axis_index_groups=groups(0)
    )


def long_way(rows, layer):
    rows = rows[:, layer * BOTH : (layer + 1) * BOTH].reshape(SIDE * BOTH, BLOCK)
    rows = lax.all_gather(rows, ("sp", "tp"), axis=0, tiled=True, axis_index_groups=groups(1))
    return rows.reshape(SIDE, SIDE, BOTH, BLOCK)


def shards(tokens, doc_ids, norm_gain, in_proj, mix_proj, out_scale):
    rows = tokens.shape[0]
    tp = lax.axis_index("tp")
    chip, core = tp // 2, tp % 2
    some_rows = short_way(in_proj, mix_proj)
    w0 = long_way(some_rows, 0)

    halo = 2 * WIN
    flags = (doc_ids + 1).astype(jnp.bfloat16)
    flag_row = jnp.pad(flags[rows - halo :], (0, BLOCK - halo)).reshape(1, BLOCK)
    tail = jnp.concatenate([tokens[rows - halo :], jnp.pad(flag_row, ((0, 15), (0, 0)))], axis=0)
    route = [(i, i + 1) for i in range(SIDE * SIDE - 1)]
    tail = lax.ppermute(tail, "sp", route)
    ext_tokens = jnp.concatenate([tail[:halo], tokens], axis=0)
    docs = jnp.concatenate([tail[halo, :halo], flags], axis=0).astype(jnp.float32)
    docs = jnp.broadcast_to(docs[:, None], (rows + halo, 128))

    gain = norm_gain.reshape(2, 8, BLOCK)
    hops = (jnp.arange(4, dtype=jnp.int32) + chip) % 4

    order = jnp.concatenate([2 * hops + core, 2 * hops + 1 - core])
    window = jnp.left_shift(jnp.int32(2), tp % 4)
    layout = [core, tp // 4, window]
    info = jnp.concatenate([order, jnp.stack([v.astype(jnp.int32) for v in layout])])
    scale = lax.dynamic_slice(out_scale, (0, tp * BLOCK), (2, BLOCK))
    partner = tp_perm(lambda t: t ^ 4)

    small = (docs, docs[WIN:], gain[0], gain[1], scale[0:1], scale[1:2], info)
    ext_tokens, small, some_rows = lax.optimization_barrier((ext_tokens, small, some_rows))
    w1 = long_way(some_rows, 1)
    docs0, docs1, gain0, gain1, scale0, scale1, info = small

    normed = normalize(all_channels(ext_tokens), info, gain0)
    pooled, mix_rows = project_pool(normed, info, docs0, w0, 48)
    other = lax.ppermute(pooled, "tp", partner)
    current = mix(pooled, other, info, scale0, mix_rows)

    normed = normalize(all_channels(current), info, gain1)
    pooled, mix_rows = project_pool(normed, info, docs1, w1, 48)
    other = lax.ppermute(pooled, "tp", partner)
    return mix(pooled, other, info, scale1, mix_rows)


def solution(mesh):
    placed = (P("sp", "tp"), P("sp"), P(), P(None, "sp", "tp"), P(None, "sp", "tp"), P())
    return jax.shard_map(
        shards, mesh=mesh, in_specs=placed, out_specs=P("sp", "tp"), check_vma=False
    )
```

```python
import jax
import jax.numpy as jnp
from jax import lax
from jax.experimental import pallas as pl
from jax.experimental.pallas import tpu as pltpu
from jax.sharding import PartitionSpec as P


D = 4096
WIN = 16
BLOCK = 512
SIDE = 8
IN_ROWS = 64
MIX_ROWS = 16
BOTH = IN_ROWS + MIX_ROWS
EPS = 1e-06

VMEM = pltpu.VMEM


def device(z, y, t):
    return ((z % SIDE) * SIDE + y % SIDE) * 8 + t


def groups(core_along_y):
    return [
        [device(a, b, t) if t % 2 == core_along_y else device(b, a, t) for b in range(SIDE)]
        for t in range(8)
        for a in range(SIDE)
    ]


def tp_perm(fn):
    return [(t, fn(t) % 8) for t in range(8)]


CORE, SIDE_OF, WINDOW = 8, 9, 10


def fetch(info_ref, gathered, lo, rows, dest, sems):
    along_z, along_y = [], []
    for z in range(SIDE):
        along_z.append(
            pltpu.make_async_copy(gathered.at[z, :, pl.ds(lo, rows), :], dest.at[z], sems.at[z])
        )
        along_y.append(
            pltpu.make_async_copy(gathered.at[:, z, pl.ds(lo, rows), :], dest.at[z], sems.at[z])
        )

    @pl.when(info_ref[CORE] == 0)
    def _():
        for c in along_z:
            c.start()

    @pl.when(info_ref[CORE] == 1)
    def _():
        for c in along_y:
            c.start()

    return along_z


def write_normed(info_ref, x_refs, gain_ref, dest, rows):
    def chunk(r, carry):
        here = pl.ds(pl.multiple_of(r * 16, 16), 16)
        values = [x_ref[i, here, :].astype(jnp.float32) for x_ref in x_refs for i in range(4)]
        total = values[0] * values[0]
        for v in values[1:]:
            total = total + v * v
        mean = jnp.sum(total, axis=1, keepdims=True) * (1.0 / D)
        scale = lax.rsqrt(mean + EPS)
        for i, v in enumerate(values):
            block = info_ref[i]
            normed = (v * scale) * gain_ref[pl.ds(block, 1), :]
            lanes = pl.ds(pl.multiple_of(block * BLOCK, BLOCK), BLOCK)
            dest[here, lanes] = normed.astype(jnp.bfloat16)
        return carry

    lax.fori_loop(0, rows // 16, chunk, 0)


def normalize(pieces, info, gain):
    rows = pieces[0].shape[1]

    def kernel(info_ref, mine_ref, theirs_ref, gain_ref, out_ref):
        write_normed(info_ref, [mine_ref, theirs_ref], gain_ref, out_ref, rows)

    return pl.pallas_call(
        kernel,
        out_shape=jax.ShapeDtypeStruct((rows, D), jnp.bfloat16),
        in_specs=[pl.BlockSpec(memory_space=pltpu.SMEM)] + [pl.BlockSpec(memory_space=VMEM)] * 3,
        out_specs=pl.BlockSpec(memory_space=VMEM),
        compiler_params=pltpu.CompilerParams(vmem_limit_bytes=16 * 1024 * 1024),
        cost_estimate=pl.CostEstimate(
            flops=200 * rows * D, bytes_accessed=4 * rows * D, transcendentals=0
        ),
        name="normalize",
    )(info, *pieces, gain)


def project_pool(normed, info, docs, weights, limit):
    rows = docs.shape[0]

    def kernel(info_ref, normed_ref, docs_ref, w_ref, out_ref, m_ref, w_all, acc, sems):
        copies = fetch(info_ref, w_ref, 0, IN_ROWS, w_all, sems.at[0])
        m_copies = fetch(info_ref, w_ref, IN_ROWS, MIX_ROWS, m_ref, sems.at[1])
        for z, c in enumerate(copies):
            c.wait()
            part = jnp.dot(
                normed_ref[:, z * BLOCK : (z + 1) * BLOCK],
                w_all[z].reshape(BLOCK, BLOCK),
                preferred_element_type=jnp.float32,
            )
            acc[...] = part if z == 0 else acc[...] + part
        own = docs_ref[...]
        masks, count = [], jnp.ones_like(own)
        for j in range(4):
            taken = (pltpu.roll(own, 2**j, 0) == own) & (2**j < info_ref[WINDOW])
            masks.append(taken)
            count = count + jnp.where(taken, pltpu.roll(count, 2**j, 0), 0.0)
        share = 1.0 / count
        for c in range(BLOCK // 128):
            lanes = pl.ds(c * 128, 128)
            proj = acc[:, lanes].astype(jnp.bfloat16).astype(jnp.float32)
            total = proj
            for j in range(4):
                total = total + jnp.where(masks[j], pltpu.roll(total, 2**j, 0), 0.0)
            pooled = total * share - proj
            out_ref[:, lanes] = pooled[WIN:].astype(jnp.bfloat16)
        for c in m_copies:
            c.wait()

    return pl.pallas_call(
        kernel,
        out_shape=[
            jax.ShapeDtypeStruct((rows - WIN, BLOCK), jnp.bfloat16),
            jax.ShapeDtypeStruct((SIDE, SIDE, MIX_ROWS, BLOCK), jnp.bfloat16),
        ],
        in_specs=[
            pl.BlockSpec(memory_space=pltpu.SMEM),
            pl.BlockSpec(memory_space=VMEM),
            pl.BlockSpec(memory_space=VMEM),
            pl.BlockSpec(memory_space=pltpu.HBM),
        ],
        out_specs=[pl.BlockSpec(memory_space=VMEM)] * 2,
        scratch_shapes=[
            VMEM((SIDE, SIDE, IN_ROWS, BLOCK), jnp.bfloat16),
            VMEM((rows, BLOCK), jnp.float32),
            pltpu.SemaphoreType.DMA((2, SIDE)),
        ],
        compiler_params=pltpu.CompilerParams(vmem_limit_bytes=limit * 1024 * 1024),
        cost_estimate=pl.CostEstimate(
            flops=2 * rows * D * BLOCK, bytes_accessed=7 * 1024 * 1024, transcendentals=0
        ),
        name="project_pool",
    )(info, normed, docs, weights)


def mix(own, other, info, scale_row, weights):
    rows = own.shape[0]

    def kernel(info_ref, own_ref, other_ref, scale_ref, w_ref, out_ref):
        side = info_ref[SIDE_OF]
        w_own = w_ref[pl.ds(4 * side, 4)].reshape(BLOCK, BLOCK)
        w_other = w_ref[pl.ds(4 * (1 - side), 4)].reshape(BLOCK, BLOCK)
        total = jnp.dot(own_ref[...], w_own, preferred_element_type=jnp.float32)
        total = total + jnp.dot(other_ref[...], w_other, preferred_element_type=jnp.float32)
        out_ref[...] = (total * scale_ref[...]).astype(jnp.bfloat16)

    return pl.pallas_call(
        kernel,
        out_shape=jax.ShapeDtypeStruct((rows, BLOCK), jnp.bfloat16),
        in_specs=[pl.BlockSpec(memory_space=pltpu.SMEM)] + [pl.BlockSpec(memory_space=VMEM)] * 4,
        out_specs=pl.BlockSpec(memory_space=VMEM),
        compiler_params=pltpu.CompilerParams(vmem_limit_bytes=16 * 1024 * 1024),
        cost_estimate=pl.CostEstimate(
            flops=4 * rows * BLOCK * BLOCK, bytes_accessed=2 * 1024 * 1024, transcendentals=0
        ),
        name="mix",
    )(info, own, other, scale_row, weights)


def all_channels(x):
    arrived = [x]
    for k in (1, 2, 3):
        arrived.append(lax.ppermute(x, "tp", tp_perm(lambda t, k=k: t - 2 * k)))
    mine = jnp.stack(arrived, axis=0)
    theirs = lax.ppermute(mine, "tp", tp_perm(lambda t: t ^ 1))
    return [mine, theirs]


def eight_copies(in_proj, mix_proj, layer):
    def kernel(in_ref, mix_ref, out_ref):
        for i in range(SIDE):
            out_ref[i, :IN_ROWS] = in_ref[0]
            out_ref[i, IN_ROWS:] = mix_ref[0]

    return pl.pallas_call(
        kernel,
        grid=(1,),
        out_shape=jax.ShapeDtypeStruct((SIDE, BOTH, BLOCK), jnp.bfloat16),
        in_specs=[
            pl.BlockSpec((1, IN_ROWS, BLOCK), lambda i: (layer, 0, 0)),
            pl.BlockSpec((1, MIX_ROWS, BLOCK), lambda i: (layer, 0, 0)),
        ],
        out_specs=pl.BlockSpec((SIDE, BOTH, BLOCK), lambda i: (0, 0, 0)),
        name="eight_copies",
    )(in_proj, mix_proj)


def gather_weights(in_proj, mix_proj, layer):
    rows = eight_copies(in_proj, mix_proj, layer)
    rows = lax.all_to_all(
        rows, ("sp", "tp"), split_axis=0, concat_axis=0, tiled=True, axis_index_groups=groups(0)
    )
    rows = rows.reshape(SIDE * BOTH, BLOCK)
    rows = lax.all_gather(rows, ("sp", "tp"), axis=0, tiled=True, axis_index_groups=groups(1))
    return rows.reshape(SIDE, SIDE, BOTH, BLOCK)


def shards(tokens, doc_ids, norm_gain, in_proj, mix_proj, out_scale):
    rows = tokens.shape[0]
    tp = lax.axis_index("tp")
    chip, core = tp // 2, tp % 2
    w0 = gather_weights(in_proj, mix_proj, 0)
    w1 = gather_weights(in_proj, mix_proj, 1)

    halo = 2 * WIN
    flags = (doc_ids + 1).astype(jnp.bfloat16)
    flag_row = jnp.pad(flags[rows - halo :], (0, BLOCK - halo)).reshape(1, BLOCK)
    tail = jnp.concatenate([tokens[rows - halo :], jnp.pad(flag_row, ((0, 15), (0, 0)))], axis=0)
    route = [(i, i + 1) for i in range(SIDE * SIDE - 1)]
    tail = lax.ppermute(tail, "sp", route)
    ext_tokens = jnp.concatenate([tail[:halo], tokens], axis=0)
    docs = jnp.concatenate([tail[halo, :halo], flags], axis=0).astype(jnp.float32)
    docs = jnp.broadcast_to(docs[:, None], (rows + halo, 128))

    gain = norm_gain.reshape(2, 8, BLOCK)
    hops = (jnp.arange(4, dtype=jnp.int32) + chip) % 4

    order = jnp.concatenate([2 * hops + core, 2 * hops + 1 - core])
    window = jnp.left_shift(jnp.int32(2), tp % 4)
    layout = [core, tp // 4, window]
    info = jnp.concatenate([order, jnp.stack([v.astype(jnp.int32) for v in layout])])
    scale = lax.dynamic_slice(out_scale, (0, tp * BLOCK), (2, BLOCK))
    partner = tp_perm(lambda t: t ^ 4)

    small = (docs, docs[WIN:], gain[0], gain[1], scale[0:1], scale[1:2], info)
    ext_tokens, small = lax.optimization_barrier((ext_tokens, small))
    docs0, docs1, gain0, gain1, scale0, scale1, info = small

    normed = normalize(all_channels(ext_tokens), info, gain0)
    pooled, mix_rows = project_pool(normed, info, docs0, w0, 48)
    other = lax.ppermute(pooled, "tp", partner)
    current = mix(pooled, other, info, scale0, mix_rows)

    normed = normalize(all_channels(current), info, gain1)
    pooled, mix_rows = project_pool(normed, info, docs1, w1, 48)
    other = lax.ppermute(pooled, "tp", partner)
    return mix(pooled, other, info, scale1, mix_rows)


def solution(mesh):
    placed = (P("sp", "tp"), P("sp"), P(), P(None, "sp", "tp"), P(None, "sp", "tp"), P())
    return jax.shard_map(
        shards, mesh=mesh, in_specs=placed, out_specs=P("sp", "tp"), check_vma=False
    )
```

```python
import jax
import jax.numpy as jnp
from jax import lax
from jax.experimental import pallas as pl
from jax.experimental.pallas import tpu as pltpu
from jax.sharding import PartitionSpec as P


D = 4096
WIN = 16
BLOCK = 512
SIDE = 8
IN_ROWS = 64
MIX_ROWS = 16
BOTH = IN_ROWS + MIX_ROWS
EPS = 1e-06

VMEM = pltpu.VMEM


def device(z, y, t):
    return ((z % SIDE) * SIDE + y % SIDE) * 8 + t


def groups(core_along_y):
    return [
        [device(a, b, t) if t % 2 == core_along_y else device(b, a, t) for b in range(SIDE)]
        for t in range(8)
        for a in range(SIDE)
    ]


def tp_perm(fn):
    return [(t, fn(t) % 8) for t in range(8)]


AXIS, SIDE_OF, WINDOW = 8, 9, 10


def fetch(info_ref, gathered, lo, rows, dest, sems):
    along_z, along_y = [], []
    for z in range(SIDE):
        along_z.append(
            pltpu.make_async_copy(gathered.at[z, :, pl.ds(lo, rows), :], dest.at[z], sems.at[z])
        )
        along_y.append(
            pltpu.make_async_copy(gathered.at[:, z, pl.ds(lo, rows), :], dest.at[z], sems.at[z])
        )

    @pl.when(info_ref[AXIS] == 0)
    def _():
        for c in along_z:
            c.start()

    @pl.when(info_ref[AXIS] == 1)
    def _():
        for c in along_y:
            c.start()

    return along_z


def write_normed(info_ref, x_refs, gain_ref, dest, rows):
    def chunk(r, carry):
        here = pl.ds(pl.multiple_of(r * 16, 16), 16)
        values = [x_ref[i, here, :].astype(jnp.float32) for x_ref in x_refs for i in range(4)]
        total = values[0] * values[0]
        for v in values[1:]:
            total = total + v * v
        mean = jnp.sum(total, axis=1, keepdims=True) * (1.0 / D)
        scale = lax.rsqrt(mean + EPS)
        for i, v in enumerate(values):
            block = info_ref[i]
            normed = (v * scale) * gain_ref[pl.ds(block, 1), :]
            lanes = pl.ds(pl.multiple_of(block * BLOCK, BLOCK), BLOCK)
            dest[here, lanes] = normed.astype(jnp.bfloat16)
        return carry

    lax.fori_loop(0, rows // 16, chunk, 0)


def normalize(pieces, info, gain):
    rows = pieces[0].shape[1]

    def kernel(info_ref, mine_ref, theirs_ref, gain_ref, out_ref):
        write_normed(info_ref, [mine_ref, theirs_ref], gain_ref, out_ref, rows)

    return pl.pallas_call(
        kernel,
        out_shape=jax.ShapeDtypeStruct((rows, D), jnp.bfloat16),
        in_specs=[pl.BlockSpec(memory_space=pltpu.SMEM)] + [pl.BlockSpec(memory_space=VMEM)] * 3,
        out_specs=pl.BlockSpec(memory_space=VMEM),
        compiler_params=pltpu.CompilerParams(vmem_limit_bytes=16 * 1024 * 1024),
        cost_estimate=pl.CostEstimate(
            flops=200 * rows * D, bytes_accessed=4 * rows * D, transcendentals=0
        ),
        name="normalize",
    )(info, *pieces, gain)


def project_pool(normed, info, docs, weights, limit):
    rows = docs.shape[0]

    def kernel(info_ref, normed_ref, docs_ref, w_ref, out_ref, m_ref, w_all, acc, sems):
        copies = fetch(info_ref, w_ref, 0, IN_ROWS, w_all, sems.at[0])
        m_copies = fetch(info_ref, w_ref, IN_ROWS, MIX_ROWS, m_ref, sems.at[1])
        for z, c in enumerate(copies):
            c.wait()
            part = jnp.dot(
                normed_ref[:, z * BLOCK : (z + 1) * BLOCK],
                w_all[z].reshape(BLOCK, BLOCK),
                preferred_element_type=jnp.float32,
            )
            acc[...] = part if z == 0 else acc[...] + part
        own = docs_ref[...]
        masks, count = [], jnp.ones_like(own)
        for j in range(4):
            taken = (pltpu.roll(own, 2**j, 0) == own) & (2**j < info_ref[WINDOW])
            masks.append(taken)
            count = count + jnp.where(taken, pltpu.roll(count, 2**j, 0), 0.0)
        share = 1.0 / count
        for c in range(BLOCK // 128):
            lanes = pl.ds(c * 128, 128)
            proj = acc[:, lanes].astype(jnp.bfloat16).astype(jnp.float32)
            total = proj
            for j in range(4):
                total = total + jnp.where(masks[j], pltpu.roll(total, 2**j, 0), 0.0)
            pooled = total * share - proj
            out_ref[:, lanes] = pooled[WIN:].astype(jnp.bfloat16)
        for c in m_copies:
            c.wait()

    return pl.pallas_call(
        kernel,
        out_shape=[
            jax.ShapeDtypeStruct((rows - WIN, BLOCK), jnp.bfloat16),
            jax.ShapeDtypeStruct((SIDE, SIDE, MIX_ROWS, BLOCK), jnp.bfloat16),
        ],
        in_specs=[
            pl.BlockSpec(memory_space=pltpu.SMEM),
            pl.BlockSpec(memory_space=VMEM),
            pl.BlockSpec(memory_space=VMEM),
            pl.BlockSpec(memory_space=pltpu.HBM),
        ],
        out_specs=[pl.BlockSpec(memory_space=VMEM)] * 2,
        scratch_shapes=[
            VMEM((SIDE, SIDE, IN_ROWS, BLOCK), jnp.bfloat16),
            VMEM((rows, BLOCK), jnp.float32),
            pltpu.SemaphoreType.DMA((2, SIDE)),
        ],
        compiler_params=pltpu.CompilerParams(vmem_limit_bytes=limit * 1024 * 1024),
        cost_estimate=pl.CostEstimate(
            flops=2 * rows * D * BLOCK, bytes_accessed=7 * 1024 * 1024, transcendentals=0
        ),
        name="project_pool",
    )(info, normed, docs, weights)


def mix(own, other, info, scale_row, weights):
    rows = own.shape[0]

    def kernel(info_ref, own_ref, other_ref, scale_ref, w_ref, out_ref):
        side = info_ref[SIDE_OF]
        w_own = w_ref[pl.ds(4 * side, 4)].reshape(BLOCK, BLOCK)
        w_other = w_ref[pl.ds(4 * (1 - side), 4)].reshape(BLOCK, BLOCK)
        total = jnp.dot(own_ref[...], w_own, preferred_element_type=jnp.float32)
        total = total + jnp.dot(other_ref[...], w_other, preferred_element_type=jnp.float32)
        out_ref[...] = (total * scale_ref[...]).astype(jnp.bfloat16)

    return pl.pallas_call(
        kernel,
        out_shape=jax.ShapeDtypeStruct((rows, BLOCK), jnp.bfloat16),
        in_specs=[pl.BlockSpec(memory_space=pltpu.SMEM)] + [pl.BlockSpec(memory_space=VMEM)] * 4,
        out_specs=pl.BlockSpec(memory_space=VMEM),
        compiler_params=pltpu.CompilerParams(vmem_limit_bytes=16 * 1024 * 1024),
        cost_estimate=pl.CostEstimate(
            flops=4 * rows * BLOCK * BLOCK, bytes_accessed=2 * 1024 * 1024, transcendentals=0
        ),
        name="mix",
    )(info, own, other, scale_row, weights)


def all_channels(x):
    arrived = [x]
    for k in (1, 2, 3):
        arrived.append(lax.ppermute(x, "tp", tp_perm(lambda t, k=k: t - 2 * k)))
    mine = jnp.stack(arrived, axis=0)
    theirs = lax.ppermute(mine, "tp", tp_perm(lambda t: t ^ 1))
    return [mine, theirs]


def eight_copies(in_proj, mix_proj, layer):
    def kernel(in_ref, mix_ref, out_ref):
        for i in range(SIDE):
            out_ref[i, :IN_ROWS] = in_ref[0]
            out_ref[i, IN_ROWS:] = mix_ref[0]

    return pl.pallas_call(
        kernel,
        grid=(1,),
        out_shape=jax.ShapeDtypeStruct((SIDE, BOTH, BLOCK), jnp.bfloat16),
        in_specs=[
            pl.BlockSpec((1, IN_ROWS, BLOCK), lambda i: (layer, 0, 0)),
            pl.BlockSpec((1, MIX_ROWS, BLOCK), lambda i: (layer, 0, 0)),
        ],
        out_specs=pl.BlockSpec((SIDE, BOTH, BLOCK), lambda i: (0, 0, 0)),
        name="eight_copies",
    )(in_proj, mix_proj)


def gather_weights(in_proj, mix_proj, layer):
    rows = eight_copies(in_proj, mix_proj, layer)
    rows = lax.all_to_all(
        rows, ("sp", "tp"), split_axis=0, concat_axis=0, tiled=True, axis_index_groups=groups(1)
    )
    rows = rows.reshape(SIDE * BOTH, BLOCK)
    rows = lax.all_gather(rows, ("sp", "tp"), axis=0, tiled=True, axis_index_groups=groups(0))
    return rows.reshape(SIDE, SIDE, BOTH, BLOCK)


def shards(tokens, doc_ids, norm_gain, in_proj, mix_proj, out_scale):
    rows = tokens.shape[0]
    tp = lax.axis_index("tp")
    chip, core = tp // 2, tp % 2
    w0 = gather_weights(in_proj, mix_proj, 0)
    w1 = gather_weights(in_proj, mix_proj, 1)

    halo = 2 * WIN
    flags = (doc_ids + 1).astype(jnp.bfloat16)
    flag_row = jnp.pad(flags[rows - halo :], (0, BLOCK - halo)).reshape(1, BLOCK)
    tail = jnp.concatenate([tokens[rows - halo :], jnp.pad(flag_row, ((0, 15), (0, 0)))], axis=0)
    route = [(i, i + 1) for i in range(SIDE * SIDE - 1)]
    tail = lax.ppermute(tail, "sp", route)
    ext_tokens = jnp.concatenate([tail[:halo], tokens], axis=0)
    docs = jnp.concatenate([tail[halo, :halo], flags], axis=0).astype(jnp.float32)
    docs = jnp.broadcast_to(docs[:, None], (rows + halo, 128))

    gain = norm_gain.reshape(2, 8, BLOCK)
    hops = (jnp.arange(4, dtype=jnp.int32) + chip) % 4

    order = jnp.concatenate([2 * hops + core, 2 * hops + 1 - core])
    window = jnp.left_shift(jnp.int32(2), tp % 4)
    layout = [1 - core, tp // 4, window]
    info = jnp.concatenate([order, jnp.stack([v.astype(jnp.int32) for v in layout])])
    scale = lax.dynamic_slice(out_scale, (0, tp * BLOCK), (2, BLOCK))
    partner = tp_perm(lambda t: t ^ 4)

    small = (docs, docs[WIN:], gain[0], gain[1], scale[0:1], scale[1:2], info)
    ext_tokens, small = lax.optimization_barrier((ext_tokens, small))
    docs0, docs1, gain0, gain1, scale0, scale1, info = small

    normed = normalize(all_channels(ext_tokens), info, gain0)
    pooled, mix_rows = project_pool(normed, info, docs0, w0, 48)
    other = lax.ppermute(pooled, "tp", partner)
    current = mix(pooled, other, info, scale0, mix_rows)

    normed = normalize(all_channels(current), info, gain1)
    pooled, mix_rows = project_pool(normed, info, docs1, w1, 48)
    other = lax.ppermute(pooled, "tp", partner)
    return mix(pooled, other, info, scale1, mix_rows)


def solution(mesh):
    placed = (P("sp", "tp"), P("sp"), P(), P(None, "sp", "tp"), P(None, "sp", "tp"), P())
    return jax.shard_map(
        shards, mesh=mesh, in_specs=placed, out_specs=P("sp", "tp"), check_vma=False
    )
```

```python
import jax
import jax.numpy as jnp
from jax import lax
from jax.experimental import pallas as pl
from jax.experimental.pallas import tpu as pltpu
from jax.sharding import PartitionSpec as P


D = 4096
WIN = 16
BLOCK = 512
SIDE = 8
IN_ROWS = 64
MIX_ROWS = 16
BOTH = IN_ROWS + MIX_ROWS
EPS = 1e-06

VMEM = pltpu.VMEM


def device(z, y, t):
    return ((z % SIDE) * SIDE + y % SIDE) * 8 + t


def groups(core_along_y):
    return [
        [device(a, b, t) if t % 2 == core_along_y else device(b, a, t) for b in range(SIDE)]
        for t in range(8)
        for a in range(SIDE)
    ]


def tp_perm(fn):
    return [(t, fn(t) % 8) for t in range(8)]


AXIS, SIDE_OF, WINDOW = 8, 9, 10


def fetch(info_ref, gathered, lo, rows, dest, sems):
    along_z, along_y = [], []
    for z in range(SIDE):
        along_z.append(
            pltpu.make_async_copy(gathered.at[z, :, pl.ds(lo, rows), :], dest.at[z], sems.at[z])
        )
        along_y.append(
            pltpu.make_async_copy(gathered.at[:, z, pl.ds(lo, rows), :], dest.at[z], sems.at[z])
        )

    @pl.when(info_ref[AXIS] == 0)
    def _():
        for c in along_z:
            c.start()

    @pl.when(info_ref[AXIS] == 1)
    def _():
        for c in along_y:
            c.start()

    return along_z


def write_normed(info_ref, x_refs, gain_ref, dest, rows):
    places = [(x_ref, i) for x_ref in x_refs for i in range(4)]

    def chunk(here):
        total = None
        for x_ref, i in places:
            v = x_ref[i, here, :].astype(jnp.float32)
            total = v * v if total is None else total + v * v
        mean = jnp.sum(total, axis=1, keepdims=True) * (1.0 / D)
        scale = lax.rsqrt(mean + EPS)
        for at, (x_ref, i) in enumerate(places):
            block = info_ref[at]
            v = x_ref[i, here, :].astype(jnp.float32)
            normed = (v * scale) * gain_ref[pl.ds(block, 1), :]
            lanes = pl.ds(pl.multiple_of(block * BLOCK, BLOCK), BLOCK)
            dest[here, lanes] = normed.astype(jnp.bfloat16)

    def pair(r, carry):
        for half in range(2):
            chunk(pl.ds(pl.multiple_of(r * 32 + half * 16, 16), 16))
        return carry

    lax.fori_loop(0, rows // 32, pair, 0)
    if rows % 32:
        chunk(pl.ds(rows - 16, 16))


def normalize(pieces, info, gain):
    rows = pieces[0].shape[1]

    def kernel(info_ref, mine_ref, theirs_ref, gain_ref, out_ref):
        write_normed(info_ref, [mine_ref, theirs_ref], gain_ref, out_ref, rows)

    return pl.pallas_call(
        kernel,
        out_shape=jax.ShapeDtypeStruct((rows, D), jnp.bfloat16),
        in_specs=[pl.BlockSpec(memory_space=pltpu.SMEM)] + [pl.BlockSpec(memory_space=VMEM)] * 3,
        out_specs=pl.BlockSpec(memory_space=VMEM),
        compiler_params=pltpu.CompilerParams(vmem_limit_bytes=16 * 1024 * 1024),
        cost_estimate=pl.CostEstimate(
            flops=200 * rows * D, bytes_accessed=4 * rows * D, transcendentals=0
        ),
        name="normalize",
    )(info, *pieces, gain)


def project_pool(normed, info, docs, weights, limit):
    rows = docs.shape[0]

    def kernel(info_ref, normed_ref, docs_ref, w_ref, out_ref, m_ref, w_all, acc, mask_ref, share_ref, sems):
        copies = fetch(info_ref, w_ref, 0, IN_ROWS, w_all, sems.at[0])
        m_copies = fetch(info_ref, w_ref, IN_ROWS, MIX_ROWS, m_ref, sems.at[1])
        own = docs_ref[...]
        count = jnp.ones_like(own)
        for j in range(4):
            taken = (pltpu.roll(own, 2**j, 0) == own) & (2**j < info_ref[WINDOW])
            mask_ref[j] = taken.astype(jnp.float32)
            count = count + jnp.where(taken, pltpu.roll(count, 2**j, 0), 0.0)
        share_ref[...] = 1.0 / count
        for z, c in enumerate(copies):
            c.wait()
            part = jnp.dot(
                normed_ref[:, z * BLOCK : (z + 1) * BLOCK],
                w_all[z].reshape(BLOCK, BLOCK),
                preferred_element_type=jnp.float32,
            )
            acc[...] = part if z == 0 else acc[...] + part
        share = share_ref[...]
        for c in range(BLOCK // 128):
            lanes = pl.ds(c * 128, 128)
            proj = acc[:, lanes].astype(jnp.bfloat16).astype(jnp.float32)
            total = proj
            for j in range(4):
                total = total + jnp.where(mask_ref[j] > 0.0, pltpu.roll(total, 2**j, 0), 0.0)
            pooled = total * share - proj
            out_ref[:, lanes] = pooled[WIN:].astype(jnp.bfloat16)
        for c in m_copies:
            c.wait()

    return pl.pallas_call(
        kernel,
        out_shape=[
            jax.ShapeDtypeStruct((rows - WIN, BLOCK), jnp.bfloat16),
            jax.ShapeDtypeStruct((SIDE, SIDE, MIX_ROWS, BLOCK), jnp.bfloat16),
        ],
        in_specs=[
            pl.BlockSpec(memory_space=pltpu.SMEM),
            pl.BlockSpec(memory_space=VMEM),
            pl.BlockSpec(memory_space=VMEM),
            pl.BlockSpec(memory_space=pltpu.HBM),
        ],
        out_specs=[pl.BlockSpec(memory_space=VMEM)] * 2,
        scratch_shapes=[
            VMEM((SIDE, SIDE, IN_ROWS, BLOCK), jnp.bfloat16),
            VMEM((rows, BLOCK), jnp.float32),
            VMEM((4, rows, 128), jnp.float32),
            VMEM((rows, 128), jnp.float32),
            pltpu.SemaphoreType.DMA((2, SIDE)),
        ],
        compiler_params=pltpu.CompilerParams(vmem_limit_bytes=limit * 1024 * 1024),
        cost_estimate=pl.CostEstimate(
            flops=2 * rows * D * BLOCK, bytes_accessed=7 * 1024 * 1024, transcendentals=0
        ),
        name="project_pool",
    )(info, normed, docs, weights)


def mix(own, other, info, scale_row, weights):
    rows = own.shape[0]

    def kernel(info_ref, own_ref, other_ref, scale_ref, w_ref, out_ref):
        side = info_ref[SIDE_OF]
        w_own = w_ref[pl.ds(4 * side, 4)].reshape(BLOCK, BLOCK)
        w_other = w_ref[pl.ds(4 * (1 - side), 4)].reshape(BLOCK, BLOCK)
        total = jnp.dot(own_ref[...], w_own, preferred_element_type=jnp.float32)
        total = total + jnp.dot(other_ref[...], w_other, preferred_element_type=jnp.float32)
        out_ref[...] = (total * scale_ref[...]).astype(jnp.bfloat16)

    return pl.pallas_call(
        kernel,
        out_shape=jax.ShapeDtypeStruct((rows, BLOCK), jnp.bfloat16),
        in_specs=[pl.BlockSpec(memory_space=pltpu.SMEM)] + [pl.BlockSpec(memory_space=VMEM)] * 4,
        out_specs=pl.BlockSpec(memory_space=VMEM),
        compiler_params=pltpu.CompilerParams(vmem_limit_bytes=16 * 1024 * 1024),
        cost_estimate=pl.CostEstimate(
            flops=4 * rows * BLOCK * BLOCK, bytes_accessed=2 * 1024 * 1024, transcendentals=0
        ),
        name="mix",
    )(info, own, other, scale_row, weights)


def all_channels(x):
    arrived = [x]
    for k in (1, 2, 3):
        arrived.append(lax.ppermute(x, "tp", tp_perm(lambda t, k=k: t - 2 * k)))
    mine = jnp.stack(arrived, axis=0)
    theirs = lax.ppermute(mine, "tp", tp_perm(lambda t: t ^ 1))
    return [mine, theirs]


def eight_copies(in_proj, mix_proj, layer):
    def kernel(in_ref, mix_ref, out_ref, sems):
        copies = []
        for i in range(SIDE):
            copies.append(pltpu.make_async_copy(in_ref.at[0], out_ref.at[i, pl.ds(0, IN_ROWS)], sems.at[0, i]))
            copies.append(
                pltpu.make_async_copy(mix_ref.at[0], out_ref.at[i, pl.ds(IN_ROWS, MIX_ROWS)], sems.at[1, i])
            )
        for c in copies:
            c.start()
        for c in copies:
            c.wait()

    return pl.pallas_call(
        kernel,
        grid=(1,),
        out_shape=jax.ShapeDtypeStruct((SIDE, BOTH, BLOCK), jnp.bfloat16),
        in_specs=[
            pl.BlockSpec((1, IN_ROWS, BLOCK), lambda i: (layer, 0, 0)),
            pl.BlockSpec((1, MIX_ROWS, BLOCK), lambda i: (layer, 0, 0)),
        ],
        out_specs=pl.BlockSpec(memory_space=pltpu.HBM),
        scratch_shapes=[pltpu.SemaphoreType.DMA((2, SIDE))],
        name="eight_copies",
    )(in_proj, mix_proj)


def gather_weights(in_proj, mix_proj, layer):
    rows = eight_copies(in_proj, mix_proj, layer)
    rows = lax.all_to_all(
        rows, ("sp", "tp"), split_axis=0, concat_axis=0, tiled=True, axis_index_groups=groups(1)
    )
    rows = rows.reshape(SIDE * BOTH, BLOCK)
    rows = lax.all_gather(rows, ("sp", "tp"), axis=0, tiled=True, axis_index_groups=groups(0))
    return rows.reshape(SIDE, SIDE, BOTH, BLOCK)


def shards(tokens, doc_ids, norm_gain, in_proj, mix_proj, out_scale):
    rows = tokens.shape[0]
    tp = lax.axis_index("tp")
    chip, core = tp // 2, tp % 2
    w0 = gather_weights(in_proj, mix_proj, 0)
    w1 = gather_weights(in_proj, mix_proj, 1)

    halo = 2 * WIN
    flags = (doc_ids + 1).astype(jnp.bfloat16)
    flag_row = jnp.pad(flags[rows - halo :], (0, BLOCK - halo)).reshape(1, BLOCK)
    tail = jnp.concatenate([tokens[rows - halo :], jnp.pad(flag_row, ((0, 15), (0, 0)))], axis=0)
    route = [(i, i + 1) for i in range(SIDE * SIDE - 1)]
    tail = lax.ppermute(tail, "sp", route)
    ext_tokens = jnp.concatenate([tail[:halo], tokens], axis=0)
    docs = jnp.concatenate([tail[halo, :halo], flags], axis=0).astype(jnp.float32)
    docs = jnp.broadcast_to(docs[:, None], (rows + halo, 128))

    gain = norm_gain.reshape(2, 8, BLOCK)
    hops = (jnp.arange(4, dtype=jnp.int32) + chip) % 4

    order = jnp.concatenate([2 * hops + core, 2 * hops + 1 - core])
    window = jnp.left_shift(jnp.int32(2), tp % 4)
    layout = [1 - core, tp // 4, window]
    info = jnp.concatenate([order, jnp.stack([v.astype(jnp.int32) for v in layout])])
    scale = lax.dynamic_slice(out_scale, (0, tp * BLOCK), (2, BLOCK))
    partner = tp_perm(lambda t: t ^ 4)

    small = (docs, docs[WIN:], gain[0], gain[1], scale[0:1], scale[1:2], info)
    ext_tokens, small = lax.optimization_barrier((ext_tokens, small))
    docs0, docs1, gain0, gain1, scale0, scale1, info = small

    normed = normalize(all_channels(ext_tokens), info, gain0)
    pooled, mix_rows = project_pool(normed, info, docs0, w0, 48)
    other = lax.ppermute(pooled, "tp", partner)
    current = mix(pooled, other, info, scale0, mix_rows)

    normed = normalize(all_channels(current), info, gain1)
    pooled, mix_rows = project_pool(normed, info, docs1, w1, 48)
    other = lax.ppermute(pooled, "tp", partner)
    return mix(pooled, other, info, scale1, mix_rows)


def solution(mesh):
    placed = (P("sp", "tp"), P("sp"), P(), P(None, "sp", "tp"), P(None, "sp", "tp"), P())
    return jax.shard_map(shards, mesh=mesh, in_specs=placed, out_specs=P("sp", "tp"), check_vma=False)
```

```python
import jax
import jax.numpy as jnp
from jax import lax
from jax.experimental import pallas as pl
from jax.experimental.pallas import tpu as pltpu
from jax.sharding import PartitionSpec as P


D = 4096
WIN = 16
BLOCK = 512
SIDE = 8
IN_ROWS = 64
MIX_ROWS = 16
BOTH = IN_ROWS + MIX_ROWS
EPS = 1e-06

VMEM = pltpu.VMEM


def device(z, y, t):
    return ((z % SIDE) * SIDE + y % SIDE) * 8 + t


def groups(core_along_y):
    return [
        [device(a, b, t) if t % 2 == core_along_y else device(b, a, t) for b in range(SIDE)]
        for t in range(8)
        for a in range(SIDE)
    ]


def tp_perm(fn):
    return [(t, fn(t) % 8) for t in range(8)]


AXIS, SIDE_OF, WINDOW = 8, 9, 10


def fetch(info_ref, gathered, lo, rows, dest, sems):
    along_z, along_y = [], []
    for z in range(SIDE):
        along_z.append(
            pltpu.make_async_copy(gathered.at[z, :, pl.ds(lo, rows), :], dest.at[z], sems.at[z])
        )
        along_y.append(
            pltpu.make_async_copy(gathered.at[:, z, pl.ds(lo, rows), :], dest.at[z], sems.at[z])
        )

    @pl.when(info_ref[AXIS] == 0)
    def _():
        for c in along_z:
            c.start()

    @pl.when(info_ref[AXIS] == 1)
    def _():
        for c in along_y:
            c.start()

    return along_z


def write_normed(info_ref, x_refs, gain_ref, dest, rows):
    places = [(x_ref, i) for x_ref in x_refs for i in range(4)]

    def chunk(here):
        total = None
        for x_ref, i in places:
            v = x_ref[i, here, :].astype(jnp.float32)
            total = v * v if total is None else total + v * v
        mean = jnp.sum(total, axis=1, keepdims=True) * (1.0 / D)
        scale = lax.rsqrt(mean + EPS)
        for at, (x_ref, i) in enumerate(places):
            block = info_ref[at]
            v = x_ref[i, here, :].astype(jnp.float32)
            normed = (v * scale) * gain_ref[pl.ds(block, 1), :]
            lanes = pl.ds(pl.multiple_of(block * BLOCK, BLOCK), BLOCK)
            dest[here, lanes] = normed.astype(jnp.bfloat16)

    def pair(r, carry):
        for half in range(2):
            chunk(pl.ds(pl.multiple_of(r * 32 + half * 16, 16), 16))
        return carry

    lax.fori_loop(0, rows // 32, pair, 0)
    if rows % 32:
        chunk(pl.ds(rows - 16, 16))


def normalize(pieces, info, gain):
    rows = pieces[0].shape[1]

    def kernel(info_ref, mine_ref, theirs_ref, gain_ref, out_ref):
        write_normed(info_ref, [mine_ref, theirs_ref], gain_ref, out_ref, rows)

    return pl.pallas_call(
        kernel,
        out_shape=jax.ShapeDtypeStruct((rows, D), jnp.bfloat16),
        in_specs=[pl.BlockSpec(memory_space=pltpu.SMEM)] + [pl.BlockSpec(memory_space=VMEM)] * 3,
        out_specs=pl.BlockSpec(memory_space=VMEM),
        compiler_params=pltpu.CompilerParams(vmem_limit_bytes=16 * 1024 * 1024),
        cost_estimate=pl.CostEstimate(
            flops=200 * rows * D, bytes_accessed=4 * rows * D, transcendentals=0
        ),
        name="normalize",
    )(info, *pieces, gain)


def project_pool(normed, info, docs, weights, limit):
    rows = docs.shape[0]

    def kernel(info_ref, normed_ref, docs_ref, w_ref, out_ref, m_ref, w_all, acc, mask_ref, share_ref, sems):
        copies = fetch(info_ref, w_ref, 0, IN_ROWS, w_all, sems.at[0])
        m_copies = fetch(info_ref, w_ref, IN_ROWS, MIX_ROWS, m_ref, sems.at[1])
        own = docs_ref[...]
        count = jnp.ones_like(own)
        for j in range(4):
            taken = (pltpu.roll(own, 2**j, 0) == own) & (2**j < info_ref[WINDOW])
            mask_ref[j] = taken.astype(jnp.float32)
            count = count + jnp.where(taken, pltpu.roll(count, 2**j, 0), 0.0)
        share_ref[...] = 1.0 / count
        for z, c in enumerate(copies):
            c.wait()
            part = jnp.dot(
                normed_ref[:, z * BLOCK : (z + 1) * BLOCK],
                w_all[z].reshape(BLOCK, BLOCK),
                preferred_element_type=jnp.float32,
            )
            acc[...] = part if z == 0 else acc[...] + part
        share = share_ref[...]
        for c in range(BLOCK // 128):
            lanes = pl.ds(c * 128, 128)
            proj = acc[:, lanes].astype(jnp.bfloat16).astype(jnp.float32)
            total = proj
            for j in range(4):
                total = total + jnp.where(mask_ref[j] > 0.0, pltpu.roll(total, 2**j, 0), 0.0)
            pooled = total * share - proj
            out_ref[:, lanes] = pooled[WIN:].astype(jnp.bfloat16)
        for c in m_copies:
            c.wait()

    return pl.pallas_call(
        kernel,
        out_shape=[
            jax.ShapeDtypeStruct((rows - WIN, BLOCK), jnp.bfloat16),
            jax.ShapeDtypeStruct((SIDE, SIDE, MIX_ROWS, BLOCK), jnp.bfloat16),
        ],
        in_specs=[
            pl.BlockSpec(memory_space=pltpu.SMEM),
            pl.BlockSpec(memory_space=VMEM),
            pl.BlockSpec(memory_space=VMEM),
            pl.BlockSpec(memory_space=pltpu.HBM),
        ],
        out_specs=[pl.BlockSpec(memory_space=VMEM)] * 2,
        scratch_shapes=[
            VMEM((SIDE, SIDE, IN_ROWS, BLOCK), jnp.bfloat16),
            VMEM((rows, BLOCK), jnp.float32),
            VMEM((4, rows, 128), jnp.float32),
            VMEM((rows, 128), jnp.float32),
            pltpu.SemaphoreType.DMA((2, SIDE)),
        ],
        compiler_params=pltpu.CompilerParams(vmem_limit_bytes=limit * 1024 * 1024),
        cost_estimate=pl.CostEstimate(
            flops=2 * rows * D * BLOCK, bytes_accessed=7 * 1024 * 1024, transcendentals=0
        ),
        name="project_pool",
    )(info, normed, docs, weights)


def mix_own(own, info, weights):
    rows = own.shape[0]

    def kernel(info_ref, own_ref, w_ref, out_ref):
        w = w_ref[pl.ds(4 * info_ref[SIDE_OF], 4)].reshape(BLOCK, BLOCK)
        out_ref[...] = jnp.dot(own_ref[...], w, preferred_element_type=jnp.float32)

    return pl.pallas_call(
        kernel,
        out_shape=jax.ShapeDtypeStruct((rows, BLOCK), jnp.float32),
        in_specs=[pl.BlockSpec(memory_space=pltpu.SMEM)] + [pl.BlockSpec(memory_space=VMEM)] * 2,
        out_specs=pl.BlockSpec(memory_space=VMEM),
        compiler_params=pltpu.CompilerParams(vmem_limit_bytes=16 * 1024 * 1024),
        cost_estimate=pl.CostEstimate(
            flops=2 * rows * BLOCK * BLOCK, bytes_accessed=2 * 1024 * 1024, transcendentals=0
        ),
        name="mix_own",
    )(info, own, weights)


def mix(part, other, info, scale_row, weights):
    rows = other.shape[0]
    half = rows // 2

    def kernel(info_ref, part_ref, other_ref, scale_ref, w_ref, out_ref, result, sems):
        w = w_ref[pl.ds(4 * (1 - info_ref[SIDE_OF]), 4)].reshape(BLOCK, BLOCK)
        copies = []
        for i in range(2):
            here = pl.ds(i * half, half)
            total = part_ref[here, :] + jnp.dot(
                other_ref[here, :], w, preferred_element_type=jnp.float32
            )
            result[i] = (total * scale_ref[...]).astype(jnp.bfloat16)
            copies.append(pltpu.make_async_copy(result.at[i], out_ref.at[here, :], sems.at[i]))
            copies[i].start()
        for c in copies:
            c.wait()

    return pl.pallas_call(
        kernel,
        out_shape=jax.ShapeDtypeStruct((rows, BLOCK), jnp.bfloat16),
        in_specs=[pl.BlockSpec(memory_space=pltpu.SMEM)] + [pl.BlockSpec(memory_space=VMEM)] * 4,
        out_specs=pl.BlockSpec(memory_space=pl.ANY),
        scratch_shapes=[VMEM((2, half, BLOCK), jnp.bfloat16), pltpu.SemaphoreType.DMA((2,))],
        compiler_params=pltpu.CompilerParams(vmem_limit_bytes=16 * 1024 * 1024),
        cost_estimate=pl.CostEstimate(
            flops=2 * rows * BLOCK * BLOCK, bytes_accessed=2 * 1024 * 1024, transcendentals=0
        ),
        name="mix",
    )(info, part, other, scale_row, weights)


def all_channels(x):
    arrived = [x]
    for k in (1, 2, 3):
        arrived.append(lax.ppermute(x, "tp", tp_perm(lambda t, k=k: t - 2 * k)))
    mine = jnp.stack(arrived, axis=0)
    theirs = lax.ppermute(mine, "tp", tp_perm(lambda t: t ^ 1))
    return [mine, theirs]


def eight_copies(in_proj, mix_proj, layer):
    def kernel(in_ref, mix_ref, out_ref, sems):
        copies = []
        for i in range(SIDE):
            copies.append(pltpu.make_async_copy(in_ref.at[0], out_ref.at[i, pl.ds(0, IN_ROWS)], sems.at[0, i]))
            copies.append(
                pltpu.make_async_copy(mix_ref.at[0], out_ref.at[i, pl.ds(IN_ROWS, MIX_ROWS)], sems.at[1, i])
            )
        for c in copies:
            c.start()
        for c in copies:
            c.wait()

    return pl.pallas_call(
        kernel,
        grid=(1,),
        out_shape=jax.ShapeDtypeStruct((SIDE, BOTH, BLOCK), jnp.bfloat16),
        in_specs=[
            pl.BlockSpec((1, IN_ROWS, BLOCK), lambda i: (layer, 0, 0)),
            pl.BlockSpec((1, MIX_ROWS, BLOCK), lambda i: (layer, 0, 0)),
        ],
        out_specs=pl.BlockSpec(memory_space=pltpu.HBM),
        scratch_shapes=[pltpu.SemaphoreType.DMA((2, SIDE))],
        name="eight_copies",
    )(in_proj, mix_proj)


def gather_weights(in_proj, mix_proj, layer):
    rows = eight_copies(in_proj, mix_proj, layer)
    rows = lax.all_to_all(
        rows, ("sp", "tp"), split_axis=0, concat_axis=0, tiled=True, axis_index_groups=groups(1)
    )
    rows = rows.reshape(SIDE * BOTH, BLOCK)
    rows = lax.all_gather(rows, ("sp", "tp"), axis=0, tiled=True, axis_index_groups=groups(0))
    return rows.reshape(SIDE, SIDE, BOTH, BLOCK)


def shards(tokens, doc_ids, norm_gain, in_proj, mix_proj, out_scale):
    rows = tokens.shape[0]
    tp = lax.axis_index("tp")
    chip, core = tp // 2, tp % 2
    w0 = gather_weights(in_proj, mix_proj, 0)
    w1 = gather_weights(in_proj, mix_proj, 1)

    halo = 2 * WIN
    flags = (doc_ids + 1).astype(jnp.bfloat16)
    flag_row = jnp.pad(flags[rows - halo :], (0, BLOCK - halo)).reshape(1, BLOCK)
    tail = jnp.concatenate([tokens[rows - halo :], jnp.pad(flag_row, ((0, 15), (0, 0)))], axis=0)
    route = [(i, i + 1) for i in range(SIDE * SIDE - 1)]
    tail = lax.ppermute(tail, "sp", route)
    ext_tokens = jnp.concatenate([tail[:halo], tokens], axis=0)
    docs = jnp.concatenate([tail[halo, :halo], flags], axis=0).astype(jnp.float32)
    docs = jnp.broadcast_to(docs[:, None], (rows + halo, 128))

    gain = norm_gain.reshape(2, 8, BLOCK)
    hops = (jnp.arange(4, dtype=jnp.int32) + chip) % 4

    order = jnp.concatenate([2 * hops + core, 2 * hops + 1 - core])
    window = jnp.left_shift(jnp.int32(2), tp % 4)
    layout = [1 - core, tp // 4, window]
    info = jnp.concatenate([order, jnp.stack([v.astype(jnp.int32) for v in layout])])
    scale = lax.dynamic_slice(out_scale, (0, tp * BLOCK), (2, BLOCK))
    partner = tp_perm(lambda t: t ^ 4)

    small = (docs, docs[WIN:], gain[0], gain[1], scale[0:1], scale[1:2], info)
    ext_tokens, small = lax.optimization_barrier((ext_tokens, small))
    docs0, docs1, gain0, gain1, scale0, scale1, info = small

    normed = normalize(all_channels(ext_tokens), info, gain0)
    pooled, mix_rows = project_pool(normed, info, docs0, w0, 48)
    other = lax.ppermute(pooled, "tp", partner)
    part = mix_own(pooled, info, mix_rows)
    current = mix(part, other, info, scale0, mix_rows)

    normed = normalize(all_channels(current), info, gain1)
    pooled, mix_rows = project_pool(normed, info, docs1, w1, 48)
    other = lax.ppermute(pooled, "tp", partner)
    part = mix_own(pooled, info, mix_rows)
    return mix(part, other, info, scale1, mix_rows)


def solution(mesh):
    placed = (P("sp", "tp"), P("sp"), P(), P(None, "sp", "tp"), P(None, "sp", "tp"), P())
    return jax.shard_map(
        shards, mesh=mesh, in_specs=placed, out_specs=P("sp", "tp"), check_vma=False
    )
```

```python
import jax
import jax.numpy as jnp
from jax import lax
from jax.experimental import pallas as pl
from jax.experimental.pallas import tpu as pltpu
from jax.sharding import PartitionSpec as P


D = 4096
WIN = 16
BLOCK = 512
SIDE = 8
IN_ROWS = 64
MIX_ROWS = 16
BOTH = IN_ROWS + MIX_ROWS
EPS = 1e-06

VMEM = pltpu.VMEM


def device(z, y, t):
    return ((z % SIDE) * SIDE + y % SIDE) * 8 + t


def groups(core_along_y):
    return [
        [device(a, b, t) if t % 2 == core_along_y else device(b, a, t) for b in range(SIDE)]
        for t in range(8)
        for a in range(SIDE)
    ]


def tp_perm(fn):
    return [(t, fn(t) % 8) for t in range(8)]


AXIS, SIDE_OF, WINDOW = 8, 9, 10


def fetch(info_ref, gathered, lo, rows, dest, sems):
    along_z, along_y = [], []
    for z in range(SIDE):
        along_z.append(
            pltpu.make_async_copy(gathered.at[z, :, pl.ds(lo, rows), :], dest.at[z], sems.at[z])
        )
        along_y.append(
            pltpu.make_async_copy(gathered.at[:, z, pl.ds(lo, rows), :], dest.at[z], sems.at[z])
        )

    @pl.when(info_ref[AXIS] == 0)
    def _():
        for c in along_z:
            c.start()

    @pl.when(info_ref[AXIS] == 1)
    def _():
        for c in along_y:
            c.start()

    return along_z


def write_normed(info_ref, x_refs, gain_ref, dest, rows):
    places = [(x_ref, i) for x_ref in x_refs for i in range(4)]

    def chunk(here):
        total = None
        for x_ref, i in places:
            v = x_ref[i, here, :].astype(jnp.float32)
            total = v * v if total is None else total + v * v
        mean = jnp.sum(total, axis=1, keepdims=True) * (1.0 / D)
        scale = lax.rsqrt(mean + EPS)
        for at, (x_ref, i) in enumerate(places):
            block = info_ref[at]
            v = x_ref[i, here, :].astype(jnp.float32)
            normed = (v * scale) * gain_ref[pl.ds(block, 1), :]
            lanes = pl.ds(pl.multiple_of(block * BLOCK, BLOCK), BLOCK)
            dest[here, lanes] = normed.astype(jnp.bfloat16)

    def pair(r, carry):
        for half in range(2):
            chunk(pl.ds(pl.multiple_of(r * 32 + half * 16, 16), 16))
        return carry

    lax.fori_loop(0, rows // 32, pair, 0)
    if rows % 32:
        chunk(pl.ds(rows - 16, 16))


def normalize(pieces, info, gain):
    rows = pieces[0].shape[1]

    def kernel(info_ref, mine_ref, theirs_ref, gain_ref, out_ref):
        write_normed(info_ref, [mine_ref, theirs_ref], gain_ref, out_ref, rows)

    return pl.pallas_call(
        kernel,
        out_shape=jax.ShapeDtypeStruct((rows, D), jnp.bfloat16),
        in_specs=[pl.BlockSpec(memory_space=pltpu.SMEM)] + [pl.BlockSpec(memory_space=VMEM)] * 3,
        out_specs=pl.BlockSpec(memory_space=VMEM),
        compiler_params=pltpu.CompilerParams(vmem_limit_bytes=16 * 1024 * 1024),
        cost_estimate=pl.CostEstimate(
            flops=200 * rows * D, bytes_accessed=4 * rows * D, transcendentals=0
        ),
        name="normalize",
    )(info, *pieces, gain)


def project_pool(normed, info, docs, weights, limit):
    rows = docs.shape[0]

    def kernel(info_ref, normed_ref, docs_ref, w_ref, out_ref, m_ref, w_all, acc, mask_ref, share_ref, sems):
        copies = fetch(info_ref, w_ref, 0, IN_ROWS, w_all, sems.at[0])
        m_copies = fetch(info_ref, w_ref, IN_ROWS, MIX_ROWS, m_ref, sems.at[1])
        own = docs_ref[...]
        count = jnp.ones_like(own)
        for j in range(4):
            taken = (pltpu.roll(own, 2**j, 0) == own) & (2**j < info_ref[WINDOW])
            mask_ref[j] = taken.astype(jnp.float32)
            count = count + jnp.where(taken, pltpu.roll(count, 2**j, 0), 0.0)
        share_ref[...] = 1.0 / count
        for z, c in enumerate(copies):
            c.wait()
            part = jnp.dot(
                normed_ref[:, z * BLOCK : (z + 1) * BLOCK],
                w_all[z].reshape(BLOCK, BLOCK),
                preferred_element_type=jnp.float32,
            )
            acc[...] = part if z == 0 else acc[...] + part
        share = share_ref[...]
        for c in range(BLOCK // 128):
            lanes = pl.ds(c * 128, 128)
            proj = acc[:, lanes].astype(jnp.bfloat16).astype(jnp.float32)
            total = proj
            for j in range(4):
                total = total + jnp.where(mask_ref[j] > 0.0, pltpu.roll(total, 2**j, 0), 0.0)
            pooled = total * share - proj
            out_ref[:, lanes] = pooled[WIN:].astype(jnp.bfloat16)
        for c in m_copies:
            c.wait()

    return pl.pallas_call(
        kernel,
        out_shape=[
            jax.ShapeDtypeStruct((rows - WIN, BLOCK), jnp.bfloat16),
            jax.ShapeDtypeStruct((SIDE, SIDE, MIX_ROWS, BLOCK), jnp.bfloat16),
        ],
        in_specs=[
            pl.BlockSpec(memory_space=pltpu.SMEM),
            pl.BlockSpec(memory_space=VMEM),
            pl.BlockSpec(memory_space=VMEM),
            pl.BlockSpec(memory_space=pltpu.HBM),
        ],
        out_specs=[pl.BlockSpec(memory_space=VMEM)] * 2,
        scratch_shapes=[
            VMEM((SIDE, SIDE, IN_ROWS, BLOCK), jnp.bfloat16),
            VMEM((rows, BLOCK), jnp.float32),
            VMEM((4, rows, 128), jnp.float32),
            VMEM((rows, 128), jnp.float32),
            pltpu.SemaphoreType.DMA((2, SIDE)),
        ],
        compiler_params=pltpu.CompilerParams(vmem_limit_bytes=limit * 1024 * 1024),
        cost_estimate=pl.CostEstimate(
            flops=2 * rows * D * BLOCK, bytes_accessed=7 * 1024 * 1024, transcendentals=0
        ),
        name="project_pool",
    )(info, normed, docs, weights)


def mix_own(own, info, weights):
    rows = own.shape[0]

    def kernel(info_ref, own_ref, w_ref, out_ref):
        w = w_ref[pl.ds(4 * info_ref[SIDE_OF], 4)].reshape(BLOCK, BLOCK)
        out_ref[...] = jnp.dot(own_ref[...], w, preferred_element_type=jnp.float32)

    return pl.pallas_call(
        kernel,
        out_shape=jax.ShapeDtypeStruct((rows, BLOCK), jnp.float32),
        in_specs=[pl.BlockSpec(memory_space=pltpu.SMEM)] + [pl.BlockSpec(memory_space=VMEM)] * 2,
        out_specs=pl.BlockSpec(memory_space=VMEM),
        compiler_params=pltpu.CompilerParams(vmem_limit_bytes=16 * 1024 * 1024),
        cost_estimate=pl.CostEstimate(
            flops=2 * rows * BLOCK * BLOCK, bytes_accessed=2 * 1024 * 1024, transcendentals=0
        ),
        name="mix_own",
    )(info, own, weights)


def mix(part, other, info, scale_row, weights, last):
    rows = other.shape[0]
    half = rows // 2

    def whole(info_ref, part_ref, other_ref, scale_ref, w_ref, out_ref):
        w = w_ref[pl.ds(4 * (1 - info_ref[SIDE_OF]), 4)].reshape(BLOCK, BLOCK)
        total = part_ref[...] + jnp.dot(other_ref[...], w, preferred_element_type=jnp.float32)
        out_ref[...] = (total * scale_ref[...]).astype(jnp.bfloat16)

    def halves(info_ref, part_ref, other_ref, scale_ref, w_ref, out_ref, result, sems):
        w = w_ref[pl.ds(4 * (1 - info_ref[SIDE_OF]), 4)].reshape(BLOCK, BLOCK)
        copies = []
        for i in range(2):
            here = pl.ds(i * half, half)
            total = part_ref[here, :] + jnp.dot(
                other_ref[here, :], w, preferred_element_type=jnp.float32
            )
            result[i] = (total * scale_ref[...]).astype(jnp.bfloat16)
            copies.append(pltpu.make_async_copy(result.at[i], out_ref.at[here, :], sems.at[i]))
            copies[i].start()
        for c in copies:
            c.wait()

    return pl.pallas_call(
        halves if last else whole,
        out_shape=jax.ShapeDtypeStruct((rows, BLOCK), jnp.bfloat16),
        in_specs=[pl.BlockSpec(memory_space=pltpu.SMEM)] + [pl.BlockSpec(memory_space=VMEM)] * 4,
        out_specs=pl.BlockSpec(memory_space=pl.ANY if last else VMEM),
        scratch_shapes=[VMEM((2, half, BLOCK), jnp.bfloat16), pltpu.SemaphoreType.DMA((2,))]
        if last
        else [],
        compiler_params=pltpu.CompilerParams(vmem_limit_bytes=16 * 1024 * 1024),
        cost_estimate=pl.CostEstimate(
            flops=2 * rows * BLOCK * BLOCK, bytes_accessed=2 * 1024 * 1024, transcendentals=0
        ),
        name="mix",
    )(info, part, other, scale_row, weights)


def all_channels(x):
    arrived = [x]
    for k in (1, 2, 3):
        arrived.append(lax.ppermute(x, "tp", tp_perm(lambda t, k=k: t - 2 * k)))
    mine = jnp.stack(arrived, axis=0)
    theirs = lax.ppermute(mine, "tp", tp_perm(lambda t: t ^ 1))
    return [mine, theirs]


def eight_copies(in_proj, mix_proj, layer):
    def kernel(in_ref, mix_ref, out_ref, sems):
        copies = []
        for i in range(SIDE):
            copies.append(pltpu.make_async_copy(in_ref.at[0], out_ref.at[i, pl.ds(0, IN_ROWS)], sems.at[0, i]))
            copies.append(
                pltpu.make_async_copy(mix_ref.at[0], out_ref.at[i, pl.ds(IN_ROWS, MIX_ROWS)], sems.at[1, i])
            )
        for c in copies:
            c.start()
        for c in copies:
            c.wait()

    return pl.pallas_call(
        kernel,
        grid=(1,),
        out_shape=jax.ShapeDtypeStruct((SIDE, BOTH, BLOCK), jnp.bfloat16),
        in_specs=[
            pl.BlockSpec((1, IN_ROWS, BLOCK), lambda i: (layer, 0, 0)),
            pl.BlockSpec((1, MIX_ROWS, BLOCK), lambda i: (layer, 0, 0)),
        ],
        out_specs=pl.BlockSpec(memory_space=pltpu.HBM),
        scratch_shapes=[pltpu.SemaphoreType.DMA((2, SIDE))],
        name="eight_copies",
    )(in_proj, mix_proj)


def gather_weights(in_proj, mix_proj, layer):
    rows = eight_copies(in_proj, mix_proj, layer)
    rows = lax.all_to_all(
        rows, ("sp", "tp"), split_axis=0, concat_axis=0, tiled=True, axis_index_groups=groups(1)
    )
    rows = rows.reshape(SIDE * BOTH, BLOCK)
    rows = lax.all_gather(rows, ("sp", "tp"), axis=0, tiled=True, axis_index_groups=groups(0))
    return rows.reshape(SIDE, SIDE, BOTH, BLOCK)


def shards(tokens, doc_ids, norm_gain, in_proj, mix_proj, out_scale):
    rows = tokens.shape[0]
    tp = lax.axis_index("tp")
    chip, core = tp // 2, tp % 2
    w0 = gather_weights(in_proj, mix_proj, 0)
    w1 = gather_weights(in_proj, mix_proj, 1)

    halo = 2 * WIN
    flags = (doc_ids + 1).astype(jnp.bfloat16)
    flag_row = jnp.pad(flags[rows - halo :], (0, BLOCK - halo)).reshape(1, BLOCK)
    tail = jnp.concatenate([tokens[rows - halo :], jnp.pad(flag_row, ((0, 15), (0, 0)))], axis=0)
    route = [(i, i + 1) for i in range(SIDE * SIDE - 1)]
    tail = lax.ppermute(tail, "sp", route)
    ext_tokens = jnp.concatenate([tail[:halo], tokens], axis=0)
    docs = jnp.concatenate([tail[halo, :halo], flags], axis=0).astype(jnp.float32)
    docs = jnp.broadcast_to(docs[:, None], (rows + halo, 128))

    gain = norm_gain.reshape(2, 8, BLOCK)
    hops = (jnp.arange(4, dtype=jnp.int32) + chip) % 4

    order = jnp.concatenate([2 * hops + core, 2 * hops + 1 - core])
    window = jnp.left_shift(jnp.int32(2), tp % 4)
    layout = [1 - core, tp // 4, window]
    info = jnp.concatenate([order, jnp.stack([v.astype(jnp.int32) for v in layout])])
    scale = lax.dynamic_slice(out_scale, (0, tp * BLOCK), (2, BLOCK))
    partner = tp_perm(lambda t: t ^ 4)

    small = (docs, docs[WIN:], gain[0], gain[1], scale[0:1], scale[1:2], info)
    ext_tokens, small = lax.optimization_barrier((ext_tokens, small))
    docs0, docs1, gain0, gain1, scale0, scale1, info = small

    normed = normalize(all_channels(ext_tokens), info, gain0)
    pooled, mix_rows = project_pool(normed, info, docs0, w0, 48)
    other = lax.ppermute(pooled, "tp", partner)
    part = mix_own(pooled, info, mix_rows)
    current = mix(part, other, info, scale0, mix_rows, False)

    normed = normalize(all_channels(current), info, gain1)
    pooled, mix_rows = project_pool(normed, info, docs1, w1, 48)
    other = lax.ppermute(pooled, "tp", partner)
    part = mix_own(pooled, info, mix_rows)
    return mix(part, other, info, scale1, mix_rows, True)


def solution(mesh):
    placed = (P("sp", "tp"), P("sp"), P(), P(None, "sp", "tp"), P(None, "sp", "tp"), P())
    return jax.shard_map(
        shards, mesh=mesh, in_specs=placed, out_specs=P("sp", "tp"), check_vma=False
    )
```
